32 devices in a mesh: sp: 8 (over z, y), tp: 4 (over x, core).
Axes of the slice: x: 2, y: 2, z: 4, core: 2. Of those that a mesh axis runs over, the one named last changes fastest.
Arguments:
- stream_in: bfloat16 [4096, 4096], P('sp', 'tp'), may hold values from -12 to 12
- norm_gain: float32 [2, 4096], replicated, may hold values from 0.1 to 1.9
- value_proj: bfloat16 [2, 4096, 4096], P(None, 'sp', 'tp'), may hold values from -0.09375 to 0.09375
- gate_proj: bfloat16 [2, 4096, 4096], P(None, 'sp', 'tp'), may hold values from -0.09375 to 0.09375
- out_proj: bfloat16 [2, 4096, 4096], P(None, 'sp', 'tp'), may hold values from -0.1875 to 0.1875
- conv_taps: float32 [2, 4, 4096], replicated, may hold values from -3 to 3
- block_gates: bfloat16 [2, 2, 2, 4096, 128], P(None, None, None, 'tp'), may hold values from -0.5 to 0.5
- forget_rate: float32 [2, 2, 4096], replicated, may hold values from 0 to 0.05, as said below
Outputs:
- stream_out: bfloat16 [4096, 4096], P('sp', 'tp')
The draws below stay inside these ranges and needn't reach their ends.
Inputs may be any that keep to these rules, and one draw needn't show every extreme that they name: `forget_rate`: positive.
All inputs are finite; a program needn't handle non-finite values.
Results may differ from the reference program's by a relative error of at most 0.025.
Values may be sent and summed in bfloat16 or wider, within the bound.
A program may use at most 192 MiB of HBM per device.

```python
import math
import jax
import jax.numpy as jnp
from jax import lax

D = 4096
W = 4096
BLK = 128
LAYERS = 2
TOK_DEV = 512
TOKENS = 4096
N_TP = 4


def draw_stream_in(key, part):
    subkeys = jax.random.split(key, 6)
    base = jax.random.normal(subkeys[0], (TOKENS, D), jnp.float32)
    phase = jax.random.uniform(subkeys[1], (), jnp.float32, -math.pi, math.pi)
    position = jnp.arange(D).astype(jnp.float32) / D
    channel_scale = jnp.exp(0.9 * jnp.cos(2.0 * math.pi * position + phase) + jax.random.uniform(subkeys[2], (D,), jnp.float32, -0.3, 0.3))
    nblocks = (TOKENS + TOK_DEV - 1) // TOK_DEV
    block_mix = jax.random.normal(subkeys[3], (nblocks, D), jnp.float32)
    block_mix = block_mix * jax.random.uniform(subkeys[4], (nblocks, 1), jnp.float32, 0.5, 3.0)
    row_block = jnp.arange(TOKENS) // TOK_DEV
    result = base * channel_scale + block_mix[row_block]
    return jnp.clip(result, -12.0, 12.0).astype(jnp.bfloat16)


def draw_forget_rate(key, part):
    subkeys = jax.random.split(key, 3)
    shape = (LAYERS, 2, W)
    keep_share = 0.5
    slow_pick = jax.random.uniform(subkeys[0], shape, jnp.float32) < keep_share
    slow_rate = jnp.exp(jax.random.uniform(subkeys[1], shape, jnp.float32, math.log(0.02), math.log(0.2))) / TOKENS
    fast_hi = max(0.012, 0.4 / TOK_DEV)
    fast_rate = jnp.exp(jax.random.uniform(subkeys[2], shape, jnp.float32, math.log(fast_hi / 4.0), math.log(fast_hi)))
    return jnp.where(slow_pick, slow_rate, fast_rate)


def block_levels(stream_key, extent, shards, smallest, top_value):
    level, own = 1.0, jax.random.fold_in(stream_key, 6)
    for dim, blocks in shards:
        draws = jnp.exp(jax.random.uniform(jax.random.fold_in(own, dim), (blocks,), jnp.float32, smallest / len(shards), top_value / len(shards)))
        level = level * jnp.repeat(draws, extent[dim] // blocks).reshape([-1 if axis == dim else 1 for axis in range(len(extent))])
    return level


def scatter_about(own_key, dims, scale, reach, pieces=(), kind=jnp.bfloat16):
    level = block_levels(own_key, dims, pieces, -0.22, 0.18) if pieces else 1.0
    array = jax.random.normal(own_key, dims, jnp.float32) * scale * level
    return jnp.minimum(jnp.maximum(array, -reach), reach).astype(kind)


def setup_inputs(seed: int = 0) -> dict:
    seeds = jax.random.split(jax.random.key(seed), 9)
    stream_in = draw_stream_in(jax.random.fold_in(seeds[8], 71), 0)
    norm_gain = jnp.clip(1.0 + 0.18 * jax.random.normal(seeds[1], (LAYERS, D), jnp.float32), 0.1, 1.9)
    value_proj = scatter_about(seeds[2], (LAYERS, D, W), D ** -0.5, 0.09375, ((1, 8), (2, 4)))
    gate_proj = scatter_about(seeds[3], (LAYERS, D, W), D ** -0.5, 0.09375, ((1, 8), (2, 4)))
    out_proj = scatter_about(seeds[4], (LAYERS, D, W), (W // 4) ** -0.5, 0.1875, ((1, 8), (2, 4)))
    conv_taps = scatter_about(seeds[5], (LAYERS, 4, W), 0.8, 3.0, (), jnp.float32)
    block_gates = scatter_about(seeds[6], (LAYERS, 2, 2, W, BLK), BLK ** -0.5, 0.5, ((3, 4),))
    forget_rate = draw_forget_rate(jax.random.fold_in(seeds[8], 71), 0)
    return dict(stream_in=stream_in, norm_gain=norm_gain, value_proj=value_proj, gate_proj=gate_proj, out_proj=out_proj, conv_taps=conv_taps, block_gates=block_gates, forget_rate=forget_rate)


GATE_SCALE = 8.0
NORM_EPS = 1e-06

def pair_combine(earlier, latter):
    return (earlier[0] * latter[0], latter[0] * earlier[1] + latter[1])

def convolve(padded, taps_layer, length):
    values = padded.astype(jnp.float32)
    return sum((values[offset:offset + length] * taps_layer[offset] for offset in range(4)))

def gate_inputs(conv_out, gate_layer):
    count, width = conv_out.shape
    block_size = gate_layer.shape[-1]
    nblocks = width // block_size
    blocked = conv_out.reshape(count, nblocks, block_size)
    weights = gate_layer.astype(jnp.float32).reshape(4, nblocks, block_size, block_size)
    pre = jnp.einsum('tnc,gncd->gtnd', blocked, weights, precision=lax.Precision.HIGHEST)
    return pre.reshape(4, count, width)

def decay_inputs(conv_out, pre, rate_layer, direction):
    recur_gate = jax.nn.sigmoid(pre[2 * direction])
    input_gate = jax.nn.sigmoid(pre[2 * direction + 1])
    log_decay = -GATE_SCALE * recur_gate * rate_layer[direction]
    decay = jnp.exp(log_decay)
    drive = jnp.sqrt(-jnp.expm1(2.0 * log_decay)) * input_gate * conv_out
    return (decay, drive)

def reference(stream_in, norm_gain, value_proj, gate_proj, out_proj, conv_taps, block_gates, forget_rate):
    stream = stream_in
    length = stream_in.shape[0]
    group_width = W // N_TP
    for layer_index in range(LAYERS):
        values = stream.astype(jnp.float32)
        scale = lax.rsqrt(lax.optimization_barrier(jnp.mean(values * values, axis=1, keepdims=True)) + NORM_EPS)
        normed = (values * scale * norm_gain[layer_index]).astype(jnp.bfloat16)
        mix_in = jnp.dot(normed, value_proj[layer_index], preferred_element_type=jnp.float32).astype(jnp.bfloat16)
        gate_z = jnp.dot(normed, gate_proj[layer_index], preferred_element_type=jnp.float32).astype(jnp.bfloat16)
        padded = jnp.pad(mix_in, ((2, 1), (0, 0)))
        conv_out = convolve(padded, conv_taps[layer_index], length)
        pre = gate_inputs(conv_out, block_gates[layer_index])
        fwd_decay, fwd_drive = decay_inputs(conv_out, pre, forget_rate[layer_index], 0)
        bwd_decay, bwd_drive = decay_inputs(conv_out, pre, forget_rate[layer_index], 1)
        _, fwd_state = lax.associative_scan(pair_combine, (fwd_decay, fwd_drive), axis=0)
        _, bwd_flip = lax.associative_scan(pair_combine, (jnp.flip(bwd_decay, 0), jnp.flip(bwd_drive, 0)), axis=0)
        both = fwd_state + jnp.flip(bwd_flip, 0)
        mixed = (both * jax.nn.silu(gate_z.astype(jnp.float32))).astype(jnp.bfloat16)
        branch = jnp.zeros((length, D), jnp.float32)
        for group in range(N_TP):
            part = lax.dot_general(mixed[:, group * group_width:(group + 1) * group_width], out_proj[layer_index][:, group * group_width:(group + 1) * group_width], (((1,), (1,)), ((), ())), preferred_element_type=jnp.float32)
            rounded = lax.optimization_barrier(part.astype(jnp.bfloat16))
            branch = branch + rounded.astype(jnp.float32)
        stream = (values + branch).astype(jnp.bfloat16)
    return stream
```

```python
import jax
import jax.numpy as jnp
from jax import lax
from jax.experimental import pallas as pl
from jax.experimental.pallas import tpu as pltpu
from jax.sharding import PartitionSpec as P

GATE_SCALE = 8.0
NORM_EPS = 1e-06
ROW_STEPS = 4
CHUNKS = 8


def solve_gates(pre_r, pre_i, rate, conv):
    recur_gate = jax.nn.sigmoid(pre_r)
    input_gate = jax.nn.sigmoid(pre_i)
    log_decay = -GATE_SCALE * recur_gate * rate
    decay = jnp.exp(log_decay)
    twice = 2.0 * log_decay
    series = jnp.ones_like(twice)
    for order in range(10, 1, -1):
        series = 1.0 + twice * (1.0 / order) * series
    loss = jnp.where(twice > -0.9, -twice * series, 1.0 - jnp.exp(twice))
    return decay, jnp.sqrt(loss) * input_gate * conv


def scan_kernel(
    mix_ref, before_ref, after_ref, taps_ref, gates_ref, rate_ref,
    both_ref, fcum_ref, bcum_ref, ends_ref,
    padded, fa, fu, ba, bu, fh, fp, bh, bp,
):
    count, width = mix_ref.shape
    padded[0:8, :] = before_ref[...].astype(jnp.float32)
    padded[8 : count + 8, :] = mix_ref[...].astype(jnp.float32)
    padded[count + 8 : count + 16, :] = after_ref[...].astype(jnp.float32)
    weights = jnp.concatenate([gates_ref[i] for i in range(4)], axis=1)
    rows = count // ROW_STEPS
    for step in range(ROW_STEPS):
        base = step * rows
        conv = padded[base + 6 : base + 6 + rows, :] * taps_ref[0:1, :]
        for tap in range(1, 4):
            conv += padded[base + 6 + tap : base + 6 + tap + rows, :] * taps_ref[tap : tap + 1, :]
        high = conv.astype(jnp.bfloat16)
        low = (conv - high.astype(jnp.float32)).astype(jnp.bfloat16)
        pre = jnp.dot(high, weights, preferred_element_type=jnp.float32)
        pre += jnp.dot(low, weights, preferred_element_type=jnp.float32)
        for e, (decay_to, drive_to) in enumerate(((fa, fu), (ba, bu))):
            decay, drive = solve_gates(
                pre[:, 2 * e * width : (2 * e + 1) * width],
                pre[:, (2 * e + 1) * width : (2 * e + 2) * width],
                rate_ref[e : e + 1, :],
                conv,
            )
            decay_to[base : base + rows, :] = decay
            drive_to[base : base + rows, :] = drive
    chunk = count // CHUNKS

    def advance(j, carry):
        f_state, f_prod, b_state, b_prod = carry
        at = pl.ds(j, CHUNKS, stride=chunk)
        back = pl.ds(chunk - 1 - j, CHUNKS, stride=chunk)
        f_decay, b_decay = fa[at, :], ba[back, :]
        f_state = f_decay * f_state + fu[at, :]
        f_prod = f_decay * f_prod
        b_state = b_decay * b_state + bu[back, :]
        b_prod = b_decay * b_prod
        fh[at, :] = f_state
        fp[at, :] = f_prod
        bh[back, :] = b_state
        bp[back, :] = b_prod
        return f_state, f_prod, b_state, b_prod

    zeros = jnp.zeros((CHUNKS, width), jnp.float32)
    ones = jnp.ones((CHUNKS, width), jnp.float32)
    f_state, f_prod, b_state, b_prod = lax.fori_loop(
        0, chunk, advance, (zeros, ones, zeros, ones), unroll=8
    )
    zero_row, one_row = zeros[0:1], ones[0:1]
    f_in, b_in = [], [None] * CHUNKS
    state, prod = zero_row, one_row
    for c in range(CHUNKS):
        f_in.append((state, prod))
        state = f_prod[c : c + 1] * state + f_state[c : c + 1]
        prod = f_prod[c : c + 1] * prod
    f_end, f_all = state, prod
    state, prod = zero_row, one_row
    for c in reversed(range(CHUNKS)):
        b_in[c] = (state, prod)
        state = b_prod[c : c + 1] * state + b_state[c : c + 1]
        prod = b_prod[c : c + 1] * prod
    ends_ref[...] = jnp.concatenate([f_all, f_end, prod, state, zeros[0:4]], axis=0)
    for c in range(CHUNKS):
        part = slice(c * chunk, (c + 1) * chunk)
        f_local, b_local = fp[part, :], bp[part, :]
        both_ref[part, :] = (
            fh[part, :] + f_local * f_in[c][0] + bh[part, :] + b_local * b_in[c][0]
        )
        fcum_ref[part, :] = f_local * f_in[c][1]
        bcum_ref[part, :] = b_local * b_in[c][1]


def local_scan(mix_in, before, after, taps_own, gates, rate_own):
    count, width = mix_in.shape
    block = gates.shape[-1]
    gates = gates.reshape(4, width, block)
    tile = pl.BlockSpec((count, block), lambda i: (0, i))
    edge = pl.BlockSpec((8, block), lambda i: (0, i))
    whole = jax.ShapeDtypeStruct((count, width), jnp.float32)
    slab = pltpu.VMEM((count, block), jnp.float32)
    return pl.pallas_call(
        scan_kernel,
        grid=(width // block,),
        in_specs=[
            tile,
            edge,
            edge,
            pl.BlockSpec((4, block), lambda i: (0, i)),
            pl.BlockSpec((4, block, block), lambda i: (0, i, 0)),
            pl.BlockSpec((2, block), lambda i: (0, i)),
        ],
        out_specs=[tile, tile, tile, edge],
        out_shape=[whole, whole, whole, jax.ShapeDtypeStruct((8, width), jnp.float32)],
        scratch_shapes=[pltpu.VMEM((count + 16, block), jnp.float32)] + [slab] * 8,
        cost_estimate=pl.CostEstimate(
            flops=count * width * 8000, bytes_accessed=count * width * 16, transcendentals=0
        ),
        name="local_scan",
    )(mix_in, before, after, taps_own, gates, rate_own)


class Layout:
    def __init__(self):
        self.sp, self.tp = lax.axis_size("sp"), lax.axis_size("tp")
        self.ny = 1 << ((self.sp.bit_length() - 1) // 2)
        self.nz = self.sp // self.ny
        self.nx = self.tp // 2
        self.groups = self.sp // 2
        rank, col = lax.axis_index("sp"), lax.axis_index("tp")
        self.z, self.y = rank // self.ny, rank % self.ny
        self.x, self.core = col // 2, col % 2
        self.role = role_of(self.z)
        self.group = (self.z // 2) * self.ny + self.y

    def z_pairs(self, k):
        return [(r, ((r // self.ny) ^ k) * self.ny + r % self.ny) for r in range(self.sp)]

    def y_pairs(self, k):
        return [
            (r, (r // self.ny) * self.ny + (r % self.ny + k) % self.ny) for r in range(self.sp)
        ]

    def x_pairs(self, k):
        return [(t, ((t // 2 + k) % self.nx) * 2 + t % 2) for t in range(self.tp)]

    def core_pairs(self):
        return [(t, t ^ 1) for t in range(self.tp)]

    def group_pairs(self, k):
        pairs = []
        for r in range(self.sp):
            z, y = r // self.ny, r % self.ny
            g = ((z // 2) * self.ny + y + k) % self.groups
            half = g // self.ny
            there = 2 * half + (role_of(z) + half) % 2
            pairs.append((r, there * self.ny + g % self.ny))
        return pairs


def role_of(z):
    return (z + z // 2) % 2


def gated(value, deps):
    deps = tuple(deps)
    if not deps:
        return value
    return lax.optimization_barrier((value, *deps))[0]


def spread_weights(at, blocks, deps):
    pieces = jnp.stack(blocks)
    pieces = gated(pieces, deps)
    own = lax.dynamic_index_in_dim(pieces, at.role, 0, keepdims=False)
    column = [(at.z, own)]
    crossed = []
    for k in range(1, at.nz):
        out = lax.dynamic_index_in_dim(pieces, role_of(at.z ^ k), 0, keepdims=False)
        got = lax.ppermute(out, "sp", at.z_pairs(k))
        column.append((at.z ^ k, got))
        crossed.append(got)
    found = [(z * at.ny + at.y, block) for z, block in column]
    for z, block in column:
        for k in range(1, at.ny):
            got = lax.ppermute(block, "sp", at.y_pairs(k))
            found.append((z * at.ny + (at.y - k) % at.ny, got))
    return found, crossed


def gather_features(at, block):
    column = [(at.x, block)]
    for k in range(1, at.nx):
        column.append(((at.x - k) % at.nx, lax.ppermute(block, "tp", at.x_pairs(k))))
    found = [(x * 2 + at.core, cells) for x, cells in column]
    for x, cells in column:
        other = lax.ppermute(cells, "tp", at.core_pairs())
        found.append((x * 2 + 1 - at.core, other))
    return found


def enter_kernel(count, owners, *refs):
    feats = refs[:count]
    gain_ref = refs[count]
    weights = refs[count + 1 : -2]
    out_ref, normed = refs[-2:]
    size = feats[0].shape[1]

    @pl.when(pl.program_id(0) == 0)
    def _():
        squares = None
        for ref in feats:
            values = ref[...].astype(jnp.float32)
            part = jnp.sum(values * values, axis=1, keepdims=True)
            squares = part if squares is None else squares + part
        scale = lax.rsqrt(squares / (size * count) + NORM_EPS)
        for i, ref in enumerate(feats):
            place = pl.ds(pl.multiple_of(owners[i] * size, 128), size)
            values = ref[...].astype(jnp.float32)
            normed[:, place] = (values * scale * gain_ref[:, place]).astype(jnp.bfloat16)

    total = None
    for i, ref in enumerate(weights):
        rows = ref.shape[0]
        place = pl.ds(pl.multiple_of(owners[count + i] * rows, 128), rows)
        term = jnp.dot(normed[:, place], ref[...], preferred_element_type=jnp.float32)
        total = term if total is None else total + term
    out_ref[...] = total.astype(jnp.bfloat16)


def enter(feats, gain, weights):
    owners = jnp.stack([t for t, _ in feats] + [r for r, _ in weights]).astype(jnp.int32)
    rows, size = feats[0][1].shape
    depth, columns = weights[0][1].shape
    width = columns // 2
    count = len(feats)
    features = size * count
    whole = pl.BlockSpec((rows, size), lambda j, _: (0, 0))
    return pl.pallas_call(
        lambda *refs: enter_kernel(count, *refs),
        grid_spec=pltpu.PrefetchScalarGridSpec(
            num_scalar_prefetch=1,
            grid=(2,),
            in_specs=[whole] * count
            + [pl.BlockSpec((1, features), lambda j, _: (0, 0))]
            + [pl.BlockSpec((depth, width), lambda j, _: (0, j))] * len(weights),
            out_specs=pl.BlockSpec((rows, width), lambda j, _: (0, j)),
            scratch_shapes=[pltpu.VMEM((rows, features), jnp.bfloat16)],
        ),
        out_shape=jax.ShapeDtypeStruct((rows, columns), jnp.bfloat16),
        cost_estimate=pl.CostEstimate(
            flops=2 * rows * features * columns,
            bytes_accessed=2 * features * (columns + rows),
            transcendentals=0,
        ),
        name="enter",
    )(owners, *[cells for _, cells in feats], gain[None, :], *[w for _, w in weights])


def leave_kernel(owners, both_ref, fcum_ref, bcum_ref, state_ref, gate_ref, *refs):
    weights, (keep_ref, give_ref, mixed) = refs[:-3], refs[-3:]
    both = both_ref[...] + fcum_ref[...] * state_ref[0:1, :] + bcum_ref[...] * state_ref[1:2, :]
    mixed[...] = (both * jax.nn.silu(gate_ref[...].astype(jnp.float32))).astype(jnp.bfloat16)
    for i, ref in enumerate(weights):
        rows = ref.shape[0]
        term = lax.dot_general(
            mixed[...], ref[...], (((1,), (1,)), ((), ())), preferred_element_type=jnp.float32
        ).astype(jnp.bfloat16)
        column = owners[3 * i]
        place = pl.ds(pl.multiple_of(owners[3 * i + 1] * rows, 128), rows)

        @pl.when(owners[3 * i + 2] == 0)
        def _():
            keep_ref[column, :, place] = term

        @pl.when(owners[3 * i + 2] != 0)
        def _():
            give_ref[column, :, place] = term


def leave(at, both, f_cum, b_cum, states, gate, weights):
    rows, width = both.shape
    depth = weights[0][1].shape[0]
    per = at.sp // at.tp
    owners = []
    for owner, _ in weights:
        t = owner // per
        owners += [(t // 2 - at.x) % at.nx, owner % per, (t % 2) ^ at.core]
    owners = jnp.stack(owners).astype(jnp.int32)
    gate_half = pl.BlockSpec((rows, width), lambda i, _: (0, 1))
    tile = pl.BlockSpec((rows, width), lambda i, _: (0, 0))
    out = pl.BlockSpec((at.nx, rows, per * depth), lambda i, _: (0, 0, 0))
    shape = jax.ShapeDtypeStruct((at.nx, rows, per * depth), jnp.bfloat16)
    return pl.pallas_call(
        leave_kernel,
        grid_spec=pltpu.PrefetchScalarGridSpec(
            num_scalar_prefetch=1,
            grid=(1,),
            in_specs=[tile] * 3
            + [pl.BlockSpec((2, width), lambda i, _: (0, 0)), gate_half]
            + [pl.BlockSpec((depth, width), lambda i, _: (0, 0))] * len(weights),
            out_specs=[out, out],
            scratch_shapes=[pltpu.VMEM((rows, width), jnp.bfloat16)],
        ),
        out_shape=[shape, shape],
        cost_estimate=pl.CostEstimate(
            flops=2 * rows * width * depth * len(weights),
            bytes_accessed=2 * rows * depth * len(weights),
            transcendentals=0,
        ),
        name="leave",
    )(owners, both, f_cum, b_cum, states, gate, *[w for _, w in weights])


def add_up(*terms):
    total = terms[0].astype(jnp.float32)
    for term in terms[1:]:
        total = total + term.astype(jnp.float32)
    return total.astype(jnp.bfloat16)


def scatter_features(at, keep, give):
    sent = []
    for k in list(range(1, at.nx)) + [0]:
        got = lax.ppermute(give[k], "tp", at.core_pairs())
        if k == 0:
            return add_up(keep[0], got, *sent)
        sent.append(lax.ppermute(add_up(keep[k], got), "tp", at.x_pairs(k)))


def all_groups(at, own):
    parts = [own]
    for k in range(1, at.groups):
        parts.append(lax.ppermute(own, "sp", at.group_pairs(k)))
    return jnp.stack(parts)


def pick(at, stacked, z, y):
    offset = (at.group - ((z // 2) * at.ny + y)) % at.groups
    sizes = (1, 1) + stacked.shape[2:]
    start = (offset, z % 2) + (0,) * (stacked.ndim - 2)
    return lax.dynamic_slice(stacked, start, sizes)[0, 0]


def by_parity(at, own, other):
    even = at.z % 2 == 0
    return jnp.stack([jnp.where(even, own, other), jnp.where(even, other, own)])


def edges_of(at, mixes):
    cut = [jnp.concatenate([m[m.shape[0] - 8 :], m[:8]]) for m in mixes]
    stacked = all_groups(at, by_parity(at, *cut))
    result = []
    for slot in range(2):
        block = (at.z ^ slot) * at.ny + at.y
        prev, succ = jnp.maximum(block - 1, 0), jnp.minimum(block + 1, at.sp - 1)
        before = pick(at, stacked, prev // at.ny, prev % at.ny)[:8]
        after = pick(at, stacked, succ // at.ny, succ % at.ny)[8:]
        before = jnp.where(block > 0, before, jnp.zeros_like(before))
        after = jnp.where(block < at.sp - 1, after, jnp.zeros_like(after))
        result.append((before, after))
    return result


def entering_states(at, ends):
    stacked = all_groups(at, by_parity(at, *ends))
    cells = [pick(at, stacked, b // at.ny, b % at.ny) for b in range(at.sp)]
    own = [(at.z ^ slot) * at.ny + at.y for slot in range(2)]
    result = []
    for block in own:
        forward = jnp.zeros_like(cells[0][0])
        backward = jnp.zeros_like(forward)
        for b in range(at.sp - 1):
            forward = jnp.where(b < block, cells[b][0] * forward + cells[b][1], forward)
        for b in range(at.sp - 1, 0, -1):
            backward = jnp.where(b > block, cells[b][2] * backward + cells[b][3], backward)
        result.append(jnp.stack([forward, backward]))
    return result


def halves(weight):
    width = weight.shape[1] // 2
    return [weight[:, :width], weight[:, width:]]


def per_device(
    stream_in, norm_gain, value_proj, gate_proj, out_proj, conv_taps, block_gates, forget_rate
):
    at = Layout()
    layers = value_proj.shape[0]
    width = value_proj.shape[2] // 2
    stream = stream_in
    first = lax.ppermute(stream, "sp", at.z_pairs(1))
    rings, deps = [], ()
    for layer in range(layers):
        joint = [
            jnp.concatenate(pair, axis=1)
            for pair in zip(halves(value_proj[layer]), halves(gate_proj[layer]))
        ]
        inward, deps = spread_weights(at, joint, deps)
        outward, deps = spread_weights(at, halves(out_proj[layer]), deps)
        rings.append((inward, outward))
    channel = (at.x * 2 + at.core) * 2 * width + at.role * width
    for layer in range(layers):
        inward, outward = rings[layer]
        partner = first if layer == 0 else lax.ppermute(stream, "sp", at.z_pairs(1))
        feats = [gather_features(at, cells) for cells in (stream, partner)]
        projected = [enter(found, norm_gain[layer], inward) for found in feats]
        mixes = [p[:, :width] for p in projected]
        edges = edges_of(at, mixes)
        taps = lax.dynamic_slice_in_dim(conv_taps[layer], channel, width, 1)
        rate = lax.dynamic_slice_in_dim(forget_rate[layer], channel, width, 1)
        gates = lax.dynamic_slice_in_dim(block_gates[layer], at.role * width, width, 2)
        scans = [
            local_scan(mix, before, after, taps, gates, rate)
            for mix, (before, after) in zip(mixes, edges)
        ]
        states = entering_states(at, [s[3] for s in scans])
        sums = [None, None]
        for slot in (1, 0):
            both, f_cum, b_cum, _ = scans[slot]
            keep, give = leave(at, both, f_cum, b_cum, states[slot], projected[slot], outward)
            sums[slot] = scatter_features(at, keep, give)
            if slot == 1:
                crossed = lax.ppermute(sums[1], "sp", at.z_pairs(1))
        stream = add_up(stream, sums[0], crossed)
    return stream


def solution(mesh):
    placed = (
        P("sp", "tp"),
        P(),
        P(None, "sp", "tp"),
        P(None, "sp", "tp"),
        P(None, "sp", "tp"),
        P(),
        P(None, None, None, "tp", None),
        P(),
    )
    return jax.shard_map(
        per_device, mesh=mesh, in_specs=placed, out_specs=P("sp", "tp"), check_vma=False
    )
```

```python
import functools

import jax
import jax.numpy as jnp
from jax import lax
from jax.experimental import pallas as pl
from jax.experimental.pallas import tpu as pltpu
from jax.sharding import PartitionSpec as P

GATE_SCALE = 8.0
NORM_EPS = 1e-06
ROW_STEPS = 4
CHUNKS = 8
MESH = pl.DeviceIdType.MESH
VMEM_BYTES = 67043328
SERIES = (1.0, -1.0 / 2, 1.0 / 6, -1.0 / 24, 1.0 / 120, -1.0 / 720, 1.0 / 5040)


def rem(a, b):
    return lax.rem(a, jnp.int32(b))


def div(a, b):
    return lax.div(a, jnp.int32(b))


def flip_bits(a, b, count):
    total, bit = 0, 1
    while bit < count:
        total = total + bit * rem(div(a, bit) + (b // bit if isinstance(b, int) else div(b, bit)), 2)
        bit *= 2
    return total


def role_of(z):
    return rem(z + div(z, 2), 2)


def sigmoid(x):
    return 0.5 * jnp.tanh(0.5 * x) + 0.5


def kernel(
    nsp, ntp, layers,
    stream_ref, value_ref, gate_ref, back_ref, gain_ref, taps_hbm, gates_hbm, rate_hbm,
    result_ref,
    feats, weights, own, mix, gate_z, padded, fa, fu, ba, bu, fh, fp, bh, bp,
    both, fcum, bcum, mixed, part, core_in, x_in, z_in, edges, ends, states, taps, gates, rate,
    start_sem, own_sem, wz_send, wy_send, w_recv,
    fz_send, fz_recv, fx_send, fx_recv, fc_send, fc_recv,
    sz_send, sz_recv, sx_send, sx_recv, sc_send, sc_recv,
    edge_send, edge_recv, end_send, end_recv, out_sem,
):
    ny = 1 << ((nsp.bit_length() - 1) // 2)
    nz, nx, groups, per = nsp // ny, ntp // 2, nsp // 2, nsp // ntp
    rank, column = lax.axis_index("sp"), lax.axis_index("tp")
    z, y, x, core = div(rank, ny), rem(rank, ny), div(column, 2), rem(column, 2)
    role = role_of(z)
    group = div(z, 2) * ny + y
    rows, width = mix.shape[1], mix.shape[2]
    depth = weights.shape[2]
    block = gates.shape[3]
    sources = (value_ref, gate_ref, back_ref)

    def z_peer(k):
        return (flip_bits(z, k, nz) * ny + y, column)

    def y_peer(k):
        return (z * ny + rem(y + k, ny), column)

    def x_peer(k):
        return (rank, rem(x + k, nx) * 2 + core)

    def group_peer(k):
        g = rem(group + k, groups)
        half = div(g, ny)
        return ((2 * half + rem(role + half, 2)) * ny + rem(g, ny), column)

    core_peer = (rank, x * 2 + 1 - core)
    peers = [z_peer(k) for k in range(1, nz)] + [y_peer(k) for k in range(1, ny)]
    peers += [x_peer(k) for k in range(1, nx)] + [core_peer]
    peers += [group_peer(k) for k in range(1, groups)]
    barrier = pltpu.get_barrier_semaphore()
    for peer in peers:
        pl.semaphore_signal(barrier, inc=1, device_id=peer, device_id_type=MESH)

    def remote(src, dst, send, recv, peer):
        return pltpu.make_async_remote_copy(
            src_ref=src, dst_ref=dst, send_sem=send, recv_sem=recv,
            device_id=peer, device_id_type=MESH,
        )

    def rows_of(m, which):
        return sources[m % 3].at[m // 3, :, pl.ds(pl.multiple_of(which * width, 128), width)]

    def own_weight(m):
        return pltpu.make_async_copy(rows_of(m, role), weights.at[m, 0], own_sem.at[m])

    def z_weight(m, k):
        there = role_of(flip_bits(z, k, nz))
        return remote(
            rows_of(m, there), weights.at[m, k * ny], wz_send.at[m, k - 1],
            w_recv.at[m, k * ny], z_peer(k),
        )

    def y_weight(m, kz, ky, first=False):
        src = rows_of(m, role) if first else weights.at[m, kz * ny]
        return remote(
            src, weights.at[m, kz * ny + ky], wy_send.at[m, kz, ky - 1],
            w_recv.at[m, kz * ny + ky], y_peer(ky),
        )

    def send_weights(ms):
        for k in range(1, nz):
            for m in ms:
                z_weight(m, k).start()

    def send_own_weights(ms):
        for m in ms:
            for ky in range(1, ny):
                y_weight(m, 0, ky, True).start()

    def relay(m, kz):
        z_weight_wait(m, kz)
        for ky in range(1, ny):
            y_weight(m, kz, ky).start()

    def z_weight_wait(m, kz):
        remote(
            weights.at[m, kz * ny], weights.at[m, kz * ny], wz_send.at[m, 0],
            w_recv.at[m, kz * ny], core_peer,
        ).wait_recv()

    def y_weight_wait(m, p):
        remote(
            weights.at[m, p], weights.at[m, p], wz_send.at[m, 0], w_recv.at[m, p], core_peer
        ).wait_recv()

    def f_copy(src, slot, at_column, send, recv, peer):
        return remote(src, feats.at[slot, at_column], send, recv, peer)

    def column_of(k):
        return rem(x + nx - k, nx) * 2 + core

    def f_to_core(slot, k, src):
        return f_copy(
            src, slot, column_of(k), fc_send.at[slot, k], fc_recv.at[slot, k], core_peer
        )

    def f_to_x(slot, k, src):
        return f_copy(
            src, slot, column, fx_send.at[slot, k - 1], fx_recv.at[slot, k - 1], x_peer(k)
        )

    def gather_start(src):
        z_copy = f_copy(src, 1, column, fz_send.at[0], fz_recv.at[0], z_peer(1))
        z_copy.start()
        for k in range(1, nx):
            f_to_x(0, k, src).start()
        f_to_core(0, 0, src).start()

    def gather_rest():
        f_copy(own, 1, column, fz_send.at[0], fz_recv.at[0], z_peer(1)).wait_recv()
        mine = feats.at[1, column]
        for k in range(1, nx):
            f_to_x(1, k, mine).start()
        f_to_core(1, 0, mine).start()
        for slot in range(2):
            for k in range(1, nx):
                there = feats.at[slot, column_of(k)]
                remote(
                    own, there, fx_send.at[slot, k - 1], fx_recv.at[slot, k - 1], core_peer
                ).wait_recv()
                f_to_core(slot, k, there).start()

    def gather_finish(slot):
        for k in range(nx):
            there = feats.at[slot, column_of(k)]
            f_to_core(slot, k, there).wait_recv()
            f_to_core(slot, k, there).wait_send()
        for k in range(1, nx):
            f_to_x(slot, k, own).wait_send()
        if slot == 1:
            f_copy(own, 1, column, fz_send.at[0], fz_recv.at[0], z_peer(1)).wait_send()

    def normalize(layer, slot):
        step = 16

        def body(i, _):
            at = pl.ds(pl.multiple_of(i * step, step), step)
            squares = None
            for t in range(ntp):
                values = feats[slot, t, at, :].astype(jnp.float32)
                total = jnp.sum(values * values, axis=1, keepdims=True)
                squares = total if squares is None else squares + total
            size = feats.shape[3]
            scale = lax.rsqrt(squares / (ntp * size) + NORM_EPS)
            for t in range(ntp):
                values = feats[slot, t, at, :].astype(jnp.float32)
                gain = gain_ref[layer : layer + 1, t * size : (t + 1) * size]
                feats[slot, t, at, :] = (values * scale * gain).astype(jnp.bfloat16)
            return 0

        lax.fori_loop(0, rows // step, body, 0)

    def owner_of(p):
        kz, ky = div(p, ny), rem(p, ny)
        return flip_bits(z, kz, nz) * ny + rem(y + ny - ky, ny)

    def enter(layer, relayed):
        fcum[...] = jnp.zeros_like(fcum)
        bcum[...] = jnp.zeros_like(bcum)
        first, second = 3 * layer, 3 * layer + 1

        def body(p, _):
            ky = rem(p, ny)
            for m in (first, second):

                @pl.when(ky != 0)
                def _():
                    y_weight_wait(m, p)

                if m not in relayed:

                    @pl.when(jnp.logical_and(ky == 0, p != 0))
                    def _():
                        relay(m, div(p, ny))

            owner = owner_of(p)
            t = div(owner, per)
            at = pl.ds(pl.multiple_of(rem(owner, per) * depth, 128), depth)
            for slot in range(2):
                cells = feats[slot, t, :, at]
                for m, total in ((first, fcum), (second, bcum)):
                    total[slot] += jnp.dot(
                        cells, weights[m, p], preferred_element_type=jnp.float32
                    )
            return 0

        for m in (first, second):
            own_weight(m).wait()
        lax.fori_loop(0, nsp, body, 0)
        for slot in range(2):
            mix[slot] = fcum[slot].astype(jnp.bfloat16)
            gate_z[slot] = bcum[slot].astype(jnp.bfloat16)

    def parity(slot):
        return rem(z + slot, 2)

    def token_block(slot):
        return flip_bits(z, slot, nz) * ny + y

    def place_of(b):
        zb, yb = div(b, ny), rem(b, ny)
        there = div(zb, 2) * ny + yb
        return rem(group + groups - there, groups), rem(zb, 2)

    def exchange(cells, send, recv):
        copies = [
            remote(cells.at[0], cells.at[k], send.at[k - 1], recv.at[k - 1], group_peer(k))
            for k in range(1, groups)
        ]
        for copy in copies:
            copy.start()
        for copy in copies:
            copy.wait_recv()
        for copy in copies:
            copy.wait_send()

    def exchange_edges():
        ends[0] = jnp.zeros(ends.shape[1:], jnp.float32)
        for slot in range(2):
            edges[0, parity(slot), 0:8, :] = mix[slot, rows - 8 : rows, :].astype(jnp.float32)
            edges[0, parity(slot), 8:16, :] = mix[slot, 0:8, :].astype(jnp.float32)
        exchange(edges, edge_send, edge_recv)

    def scan(layer, services):
        blocks = width // block
        chunk = rows // CHUNKS
        size = rows // ROW_STEPS

        def body(i, _):
            for when, m, kz in services:

                @pl.when(i == when)
                def _():
                    relay(m, kz)

            slot, b = div(i, blocks), rem(i, blocks)
            lanes = pl.ds(pl.multiple_of(b * block, 128), block)
            where = flip_bits(z, slot, nz) * ny + y
            even = rem(z + slot, 2)
            off, par = place_of(jnp.maximum(where - 1, 0))
            padded[0:8, :] = jnp.where(where > 0, edges[off, par, 0:8, lanes], 0.0)
            off, par = place_of(jnp.minimum(where + 1, nsp - 1))
            padded[rows + 8 : rows + 16, :] = jnp.where(
                where < nsp - 1, edges[off, par, 8:16, lanes], 0.0
            )
            padded[8 : rows + 8, :] = mix[slot, :, lanes].astype(jnp.float32)
            maps = jnp.concatenate([gates[layer, g, lanes, :] for g in range(4)], axis=1)
            maps = jnp.concatenate([maps, maps], axis=0)
            for step in range(ROW_STEPS):
                base = step * size
                conv = padded[base + 6 : base + 6 + size, :] * taps[layer, 0:1, lanes]
                for tap in range(1, 4):
                    conv += (
                        padded[base + 6 + tap : base + 6 + tap + size, :]
                        * taps[layer, tap : tap + 1, lanes]
                    )
                high = conv.astype(jnp.bfloat16)
                low = (conv - high.astype(jnp.float32)).astype(jnp.bfloat16)
                pre = jnp.dot(
                    jnp.concatenate([high, low], axis=1), maps, preferred_element_type=jnp.float32
                )
                for e, (decay_to, drive_to) in enumerate(((fa, fu), (ba, bu))):
                    pre_r = pre[:, 2 * e * block : (2 * e + 1) * block]
                    pre_i = pre[:, (2 * e + 1) * block : (2 * e + 2) * block]
                    speed = GATE_SCALE * rate[layer, e : e + 1, lanes]
                    fall = sigmoid(pre_r) * speed
                    series = jnp.full_like(fall, SERIES[-1])
                    for term in reversed(SERIES[:-1]):
                        series = series * fall + term
                    lost = fall * series
                    loss = lost * (2.0 - lost)
                    root = loss * lax.rsqrt(jnp.maximum(loss, 1e-30))
                    decay_to[base : base + size, :] = 1.0 - lost
                    drive_to[base : base + size, :] = root * sigmoid(pre_i) * conv

            def advance(j, carry):
                f_state, f_prod, b_state, b_prod = carry
                at = pl.ds(j, CHUNKS, stride=chunk)
                back = pl.ds(chunk - 1 - j, CHUNKS, stride=chunk)
                f_decay, b_decay = fa[at, :], ba[back, :]
                f_state = f_decay * f_state + fu[at, :]
                f_prod = f_decay * f_prod
                b_state = b_decay * b_state + bu[back, :]
                b_prod = b_decay * b_prod
                fh[at, :] = f_state
                fp[at, :] = f_prod
                bh[back, :] = b_state
                bp[back, :] = b_prod
                return f_state, f_prod, b_state, b_prod

            zeros = jnp.zeros((CHUNKS, block), jnp.float32)
            ones = jnp.ones((CHUNKS, block), jnp.float32)
            f_state, f_prod, b_state, b_prod = lax.fori_loop(
                0, chunk, advance, (zeros, ones, zeros, ones), unroll=8
            )
            f_in, b_in = [], [None] * CHUNKS
            state, prod = zeros[0:1], ones[0:1]
            for c in range(CHUNKS):
                f_in.append((state, prod))
                state = f_prod[c : c + 1] * state + f_state[c : c + 1]
                prod = f_prod[c : c + 1] * prod
            ends[0, even, 0:1, lanes] = prod
            ends[0, even, 1:2, lanes] = state
            state, prod = zeros[0:1], ones[0:1]
            for c in reversed(range(CHUNKS)):
                b_in[c] = (state, prod)
                state = b_prod[c : c + 1] * state + b_state[c : c + 1]
                prod = b_prod[c : c + 1] * prod
            ends[0, even, 2:3, lanes] = prod
            ends[0, even, 3:4, lanes] = state
            for c in range(CHUNKS):
                at = slice(c * chunk, (c + 1) * chunk)
                f_local, b_local = fp[at, :], bp[at, :]
                both[slot, at, lanes] = (
                    fh[at, :] + f_local * f_in[c][0] + bh[at, :] + b_local * b_in[c][0]
                )
                fcum[slot, at, lanes] = f_local * f_in[c][1]
                bcum[slot, at, lanes] = b_local * b_in[c][1]
            return 0

        lax.fori_loop(0, 2 * blocks, body, 0)

    def exchange_ends():
        exchange(ends, end_send, end_recv)
        for slot in range(2):
            where = token_block(slot)
            forward = jnp.zeros((1, width), jnp.float32)
            backward = jnp.zeros((1, width), jnp.float32)
            for b in range(nsp - 1):
                off, par = place_of(jnp.int32(b))
                moved = ends[off, par, 0:1, :] * forward + ends[off, par, 1:2, :]
                forward = jnp.where(where > b, moved, forward)
            for b in range(nsp - 1, 0, -1):
                off, par = place_of(jnp.int32(b))
                moved = ends[off, par, 2:3, :] * backward + ends[off, par, 3:4, :]
                backward = jnp.where(where < b, moved, backward)
            states[slot, 0:1, :] = forward
            states[slot, 1:2, :] = backward

    def leave(layer, slot, first):
        step = 32
        m = 3 * layer + 2

        def finish(i, _):
            at = pl.ds(pl.multiple_of(i * step, step), step)
            total = both[slot, at, :] + fcum[slot, at, :] * states[slot, 0:1, :]
            total = total + bcum[slot, at, :] * states[slot, 1:2, :]
            gate = gate_z[slot, at, :].astype(jnp.float32)
            mixed[at, :] = (total * gate * sigmoid(gate)).astype(jnp.bfloat16)
            return 0

        lax.fori_loop(0, rows // step, finish, 0)

        def body(p, _):
            if first:

                @pl.when(rem(p, ny) != 0)
                def _():
                    y_weight_wait(m, p)

            term = lax.dot_general(
                mixed[...], weights[m, p], (((1,), (1,)), ((), ())),
                preferred_element_type=jnp.float32,
            )
            owner = owner_of(p)
            t = div(owner, per)
            far = rem(div(t, 2) + nx - x, nx)
            other = rem(t + core, 2)
            at = pl.ds(pl.multiple_of(rem(owner, per) * depth, 128), depth)
            part[slot, other, far, :, at] = term.astype(jnp.bfloat16)
            return 0

        if first:
            own_weight(m).wait()
        lax.fori_loop(0, nsp, body, 0)

    def s_to_core(slot, k):
        return remote(
            part.at[slot, 1, k], core_in.at[slot, k], sc_send.at[slot, k], sc_recv.at[slot, k],
            core_peer,
        )

    def s_to_x(slot, k):
        return remote(
            part.at[slot, 0, k], x_in.at[slot, k - 1], sx_send.at[slot, k - 1],
            sx_recv.at[slot, k - 1], x_peer(k),
        )

    def s_to_z():
        return remote(part.at[1, 0, 0], z_in, sz_send.at[0], sz_recv.at[0], z_peer(1))

    def give(slot):
        for k in list(range(1, nx)) + [0]:
            s_to_core(slot, k).start()

    def tiles(body):
        step = 32

        def run(i, _):
            body(pl.ds(pl.multiple_of(i * step, step), step))
            return 0

        lax.fori_loop(0, rows // step, run, 0)

    def pass_on(slot):
        for k in range(1, nx):
            s_to_core(slot, k).wait_recv()

            def body(at):
                total = part[slot, 0, k, at, :].astype(jnp.float32)
                total = total + core_in[slot, k, at, :].astype(jnp.float32)
                part[slot, 0, k, at, :] = total.astype(jnp.bfloat16)

            tiles(body)
            s_to_x(slot, k).start()
        s_to_core(slot, 0).wait_recv()

    def summed(slot, at):
        total = part[slot, 0, 0, at, :].astype(jnp.float32)
        total = total + core_in[slot, 0, at, :].astype(jnp.float32)
        for k in range(1, nx):
            total = total + x_in[slot, k - 1, at, :].astype(jnp.float32)
        return total

    def land(slot):
        for k in range(1, nx):
            s_to_x(slot, k).wait_recv()

    def drain(slot):
        for k in range(nx):
            s_to_core(slot, k).wait_send()
        for k in range(1, nx):
            s_to_x(slot, k).wait_send()

    first_own = pltpu.make_async_copy(stream_ref, own, start_sem.at[0])
    first_feat = pltpu.make_async_copy(stream_ref, feats.at[0, column], start_sem.at[1])
    channel = pl.multiple_of(column * 2 * width + role * width, 128)
    small = [
        pltpu.make_async_copy(taps_hbm.at[:, :, pl.ds(channel, width)], taps, start_sem.at[2]),
        pltpu.make_async_copy(rate_hbm.at[:, :, pl.ds(channel, width)], rate, start_sem.at[3]),
        pltpu.make_async_copy(
            gates_hbm.at[:, :, pl.ds(pl.multiple_of(role * width, 128), width), :],
            gates, start_sem.at[4],
        ),
    ]
    first_own.start()
    first_feat.start()
    pl.semaphore_wait(barrier, len(peers))
    gather_start(stream_ref)
    send_weights((0, 1))
    send_own_weights((0, 1))
    for m in range(3 * layers):
        own_weight(m).start()
    for copy in small:
        copy.start()
    send_weights((2,))
    send_own_weights((2,))

    for layer in range(layers):
        last = layer == layers - 1
        gather_rest()
        if layer == 0:
            first_own.wait()
            first_feat.wait()
        for slot in range(2):
            gather_finish(slot)
            normalize(layer, slot)
        enter(layer, () if layer == 0 else (3 * layer,))
        exchange_edges()
        if not last:
            send_weights((3 * layer + 3,))
            send_own_weights((3 * layer + 3,))
        if layer == 0:
            for copy in small:
                copy.wait()
        blocks = 2 * (width // block)
        services = [
            (min(blocks - 1, (blocks * (k + 1)) // (nz + 1)), 3 * layer + 2, k)
            for k in range(1, nz)
        ]
        scan(layer, services)
        exchange_ends()
        leave(layer, 1, True)
        give(1)
        leave(layer, 0, False)
        pass_on(1)
        give(0)
        pass_on(0)
        if not last:
            for k in range(1, nz):
                relay(3 * layer + 3, k)
        land(1)

        def send_over(at):
            part[1, 0, 0, at, :] = summed(1, at).astype(jnp.bfloat16)

        tiles(send_over)
        s_to_z().start()
        land(0)
        s_to_z().wait_recv()

        def renew(at):
            total = summed(0, at) + z_in[at, :].astype(jnp.float32)
            fresh = (own[at, :].astype(jnp.float32) + total).astype(jnp.bfloat16)
            own[at, :] = fresh
            if not last:
                feats[0, column, at, :] = fresh

        tiles(renew)
        if not last:
            gather_start(own)
            send_weights((3 * layer + 4, 3 * layer + 5))
            send_own_weights((3 * layer + 4, 3 * layer + 5))
        drain(1)
        drain(0)
        s_to_z().wait_send()
    result = pltpu.make_async_copy(own, result_ref, out_sem.at[0])
    result.start()
    for m in range(3 * layers):
        for k in range(1, nz):
            z_weight(m, k).wait_send()
        for kz in range(nz):
            for ky in range(1, ny):
                y_weight(m, kz, ky, kz == 0).wait_send()
    result.wait()


def per_device(
    stream_in, norm_gain, value_proj, gate_proj, out_proj, conv_taps, block_gates, forget_rate
):
    nsp, ntp = lax.axis_size("sp"), lax.axis_size("tp")
    layers, depth, both_roles = value_proj.shape
    rows, size = stream_in.shape
    width = both_roles // 2
    block = block_gates.shape[-1]
    ny = 1 << ((nsp.bit_length() - 1) // 2)
    nz, nx, groups = nsp // ny, ntp // 2, nsp // 2
    maps = block_gates.reshape(layers, 4, both_roles, block)
    half, full = jnp.bfloat16, jnp.float32
    dma = pltpu.SemaphoreType.DMA
    slab = pltpu.VMEM((rows, block), full)
    scratch = [
        pltpu.VMEM((2, ntp, rows, size), half),
        pltpu.VMEM((3 * layers, nsp, depth, width), half),
        pltpu.VMEM((rows, size), half),
        pltpu.VMEM((2, rows, width), half),
        pltpu.VMEM((2, rows, width), half),
        pltpu.VMEM((rows + 16, block), full),
        *[slab] * 8,
        *[pltpu.VMEM((2, rows, width), full)] * 3,
        pltpu.VMEM((rows, width), half),
        pltpu.VMEM((2, 2, nx, rows, size), half),
        pltpu.VMEM((2, nx, rows, size), half),
        pltpu.VMEM((2, nx - 1, rows, size), half),
        pltpu.VMEM((rows, size), half),
        pltpu.VMEM((groups, 2, 16, width), full),
        pltpu.VMEM((groups, 2, 8, width), full),
        pltpu.VMEM((2, 8, width), full),
        pltpu.VMEM((layers, 4, width), full),
        pltpu.VMEM((layers, 4, width, block), half),
        pltpu.VMEM((layers, 2, width), full),
        dma((5,)),
        dma((3 * layers,)),
        dma((3 * layers, nz - 1)),
        dma((3 * layers, nz, ny - 1)),
        dma((3 * layers, nsp)),
        dma((1,)), dma((1,)), dma((2, nx - 1)), dma((2, nx - 1)), dma((2, nx)), dma((2, nx)),
        dma((1,)), dma((1,)), dma((2, nx - 1)), dma((2, nx - 1)), dma((2, nx)), dma((2, nx)),
        dma((groups - 1,)), dma((groups - 1,)), dma((groups - 1,)), dma((groups - 1,)),
        dma((1,)),
    ]
    anywhere = pl.BlockSpec(memory_space=pl.ANY)
    inside = pl.BlockSpec(memory_space=pltpu.VMEM)
    return pl.pallas_call(
        functools.partial(kernel, nsp, ntp, layers),
        out_shape=jax.ShapeDtypeStruct((rows, size), half),
        in_specs=[anywhere] * 4 + [inside] + [anywhere] * 3,
        out_specs=anywhere,
        scratch_shapes=scratch,
        compiler_params=pltpu.CompilerParams(
            collective_id=0, has_side_effects=True, vmem_limit_bytes=VMEM_BYTES
        ),
        name="layers",
    )(stream_in, value_proj, gate_proj, out_proj, norm_gain, conv_taps, maps, forget_rate)


def solution(mesh):
    placed = (
        P("sp", "tp"),
        P(),
        P(None, "sp", "tp"),
        P(None, "sp", "tp"),
        P(None, "sp", "tp"),
        P(),
        P(None, None, None, "tp", None),
        P(),
    )
    return jax.shard_map(
        per_device, mesh=mesh, in_specs=placed, out_specs=P("sp", "tp"), check_vma=False
    )
```

```python
import functools

import jax
import jax.numpy as jnp
from jax import lax
from jax.experimental import pallas as pl
from jax.experimental.pallas import tpu as pltpu
from jax.sharding import PartitionSpec as P

GATE_SCALE = 8.0
NORM_EPS = 1e-06
ROW_STEPS = 4
CHUNKS = 8
MESH = pl.DeviceIdType.MESH
VMEM_BYTES = 67043328
SERIES = (1.0, -1.0 / 2, 1.0 / 6, -1.0 / 24, 1.0 / 120, -1.0 / 720, 1.0 / 5040)


def rem(a, b):
    return lax.rem(a, jnp.int32(b))


def div(a, b):
    return lax.div(a, jnp.int32(b))


def flip_bits(a, b, count):
    total, bit = 0, 1
    while bit < count:
        total = total + bit * rem(div(a, bit) + (b // bit if isinstance(b, int) else div(b, bit)), 2)
        bit *= 2
    return total


def role_of(z):
    return rem(z + div(z, 2), 2)


def sigmoid(x):
    return 0.5 * jnp.tanh(0.5 * x) + 0.5


def kernel(
    nsp, ntp, layers,
    stream_ref, value_ref, gate_ref, back_ref, gain_ref, taps_hbm, gates_hbm, rate_hbm,
    result_ref,
    feats, weights, own, mix, gate_z, padded, fa, fu, ba, bu, fh, fp, bh, bp,
    both, cums, mixed, part, core_in, x_in, z_in, edges, ends, states, taps, gates, rate,
    start_sem, own_sem, wz_send, wy_send, w_recv,
    fz_send, fz_recv, fx_send, fx_recv, fc_send, fc_recv,
    sz_send, sz_recv, sx_send, sx_recv, sc_send, sc_recv,
    edge_send, edge_recv, end_send, end_recv, out_sem,
):
    ny = 1 << ((nsp.bit_length() - 1) // 2)
    nz, nx, groups, per = nsp // ny, ntp // 2, nsp // 2, nsp // ntp
    rank, column = lax.axis_index("sp"), lax.axis_index("tp")
    z, y, x, core = div(rank, ny), rem(rank, ny), div(column, 2), rem(column, 2)
    role = role_of(z)
    group = div(z, 2) * ny + y
    rows, width = mix.shape[1], mix.shape[2]
    depth = weights.shape[2]
    block = gates.shape[3]
    sources = (value_ref, gate_ref, back_ref)

    def z_peer(k):
        return (flip_bits(z, k, nz) * ny + y, column)

    def y_peer(k):
        return (z * ny + rem(y + k, ny), column)

    def x_peer(k):
        return (rank, rem(x + k, nx) * 2 + core)

    def group_peer(k):
        g = rem(group + k, groups)
        half = div(g, ny)
        return ((2 * half + rem(role + half, 2)) * ny + rem(g, ny), column)

    core_peer = (rank, x * 2 + 1 - core)
    peers = [z_peer(k) for k in range(1, nz)] + [y_peer(k) for k in range(1, ny)]
    peers += [x_peer(k) for k in range(1, nx)] + [core_peer]
    peers += [group_peer(k) for k in range(1, groups)]
    barrier = pltpu.get_barrier_semaphore()
    for peer in peers:
        pl.semaphore_signal(barrier, inc=1, device_id=peer, device_id_type=MESH)

    def remote(src, dst, send, recv, peer):
        return pltpu.make_async_remote_copy(
            src_ref=src, dst_ref=dst, send_sem=send, recv_sem=recv,
            device_id=peer, device_id_type=MESH,
        )

    def rows_of(m, which):
        return sources[m % 3].at[m // 3, :, pl.ds(pl.multiple_of(which * width, 128), width)]

    def own_weight(m):
        return pltpu.make_async_copy(rows_of(m, role), weights.at[m, 0], own_sem.at[m])

    def z_weight(m, k):
        there = role_of(flip_bits(z, k, nz))
        return remote(
            rows_of(m, there), weights.at[m, k * ny], wz_send.at[m, k - 1],
            w_recv.at[m, k * ny], z_peer(k),
        )

    def y_weight(m, kz, ky, first=False):
        src = rows_of(m, role) if first else weights.at[m, kz * ny]
        return remote(
            src, weights.at[m, kz * ny + ky], wy_send.at[m, kz, ky - 1],
            w_recv.at[m, kz * ny + ky], y_peer(ky),
        )

    def send_weights(*pairs):
        for m, k in pairs:
            z_weight(m, k).start()

    def send_own_weights(ms):
        for m in ms:
            for ky in range(1, ny):
                y_weight(m, 0, ky, True).start()

    def relay(m, kz):
        z_weight_wait(m, kz)
        for ky in range(1, ny):
            y_weight(m, kz, ky).start()

    def z_weight_wait(m, kz):
        remote(
            weights.at[m, kz * ny], weights.at[m, kz * ny], wz_send.at[m, 0],
            w_recv.at[m, kz * ny], core_peer,
        ).wait_recv()

    def y_weight_wait(m, p):
        remote(
            weights.at[m, p], weights.at[m, p], wz_send.at[m, 0], w_recv.at[m, p], core_peer
        ).wait_recv()

    def f_copy(src, slot, at_column, send, recv, peer):
        return remote(src, feats.at[slot, at_column], send, recv, peer)

    def column_of(k):
        return rem(x + nx - k, nx) * 2 + core

    def f_to_core(slot, k, src):
        return f_copy(
            src, slot, column_of(k), fc_send.at[slot, k], fc_recv.at[slot, k], core_peer
        )

    def f_to_x(slot, k, src):
        return f_copy(
            src, slot, column, fx_send.at[slot, k - 1], fx_recv.at[slot, k - 1], x_peer(k)
        )

    def f_to_z(src):
        return f_copy(src, 1, column, fz_send.at[0], fz_recv.at[0], z_peer(1))

    def gather_start(src):
        for k in range(1, nx):
            f_to_x(0, k, src).start()
        f_to_core(0, 0, src).start()

    def gather_z():
        f_to_z(own).wait_recv()
        mine = feats.at[1, column]
        for k in range(1, nx):
            f_to_x(1, k, mine).start()
        f_to_core(1, 0, mine).start()

    def gather_x(slot):
        for k in range(1, nx):
            there = feats.at[slot, column_of(k)]
            remote(
                own, there, fx_send.at[slot, k - 1], fx_recv.at[slot, k - 1], core_peer
            ).wait_recv()
            f_to_core(slot, k, there).start()

    def gather_finish(slot):
        for k in range(nx):
            there = feats.at[slot, column_of(k)]
            f_to_core(slot, k, there).wait_recv()
            f_to_core(slot, k, there).wait_send()
        for k in range(1, nx):
            f_to_x(slot, k, own).wait_send()
        if slot == 1:
            f_to_z(own).wait_send()

    def normalize(layer, slot):
        step = 16

        def body(i, _):
            at = pl.ds(pl.multiple_of(i * step, step), step)
            squares = None
            for t in range(ntp):
                values = feats[slot, t, at, :].astype(jnp.float32)
                total = jnp.sum(values * values, axis=1, keepdims=True)
                squares = total if squares is None else squares + total
            size = feats.shape[3]
            scale = lax.rsqrt(squares / (ntp * size) + NORM_EPS)
            for t in range(ntp):
                values = feats[slot, t, at, :].astype(jnp.float32)
                gain = gain_ref[layer : layer + 1, t * size : (t + 1) * size]
                feats[slot, t, at, :] = (values * scale * gain).astype(jnp.bfloat16)
            return 0

        lax.fori_loop(0, rows // step, body, 0, unroll=2)

    def owner_of(kz, ky):
        return flip_bits(z, kz, nz) * ny + rem(y + ny - ky, ny)

    def table(j, values):
        found = jnp.int32(values[0])
        for i, value in enumerate(values):
            found = jnp.where(j == i, jnp.int32(value), found)
        return found

    def nth(i):
        return jnp.where(role == 1, jnp.int32(nz - 1 - i), jnp.int32(1 + i))

    def all_steps(ms, order):
        steps = [(m, kz, 0, None) for m in ms for kz in order]
        return steps + [(m, kz, ky, None) for m in ms for kz in order for ky in range(1, ny)]

    def late_steps(m):
        order = [(0, 0)] + [(k, nz - k) for k in range(1, nz)]
        steps = [(m, kz, 0, inner) for kz, inner in order]
        return steps + [(m, kz, ky, inner) for kz, inner in order for ky in range(1, ny)]

    def walk(steps, relays, waits, use, inner_relays=()):
        steps = [(m, kz, ky, kz if inner is None else inner) for m, kz, ky, inner in steps]
        columns = list(zip(*steps))
        passing = [int(ky == 0 and kz != 0 and (m, kz) in relays) for m, kz, ky, _ in steps]
        inside = [int(ky == 0 and kz != 0 and (m, kz) in inner_relays) for m, kz, ky, _ in steps]
        waiting = [int(waits and ky != 0) for _, _, ky, _ in steps]

        def body(j, _):
            m, outer, ky, inner = [table(j, column) for column in columns]
            kz = jnp.where(role == 1, inner, outer)

            if any(passing):

                @pl.when(table(j, passing) == 1)
                def _():
                    relay(m, kz)

            if any(waiting):

                @pl.when(table(j, waiting) == 1)
                def _():
                    y_weight_wait(m, kz * ny + ky)

            if any(inside):

                @pl.when(jnp.logical_and(role == 1, table(j, inside) == 1))
                def _():
                    relay(m, kz)

            use(m, kz, ky)
            return 0

        lax.fori_loop(0, len(steps), body, 0)

    def clear(layer):
        cums[...] = jnp.zeros_like(cums)
        for m in (3 * layer, 3 * layer + 1):
            own_weight(m).wait()

    def enter(layer, slots, steps, relays, waits, inner_relays=()):
        def use(m, kz, ky):
            owner = owner_of(kz, ky)
            t = div(owner, per)
            at = pl.ds(pl.multiple_of(rem(owner, per) * depth, 128), depth)
            for slot in slots:
                cums[m - 3 * layer, slot] += jnp.dot(
                    feats[slot, t, :, at], weights[m, kz * ny + ky],
                    preferred_element_type=jnp.float32,
                )

        walk(steps, relays, waits, use, inner_relays)
        for slot in slots:
            mix[slot] = cums[0, slot].astype(jnp.bfloat16)
            gate_z[slot] = cums[1, slot].astype(jnp.bfloat16)

    def parity(slot):
        return rem(z + slot, 2)

    def token_block(slot):
        return flip_bits(z, slot, nz) * ny + y

    def place_of(b):
        zb, yb = div(b, ny), rem(b, ny)
        there = div(zb, 2) * ny + yb
        return rem(group + groups - there, groups), rem(zb, 2)

    def swaps(cells, send, recv):
        return [
            remote(cells.at[0], cells.at[k], send.at[k - 1], recv.at[k - 1], group_peer(k))
            for k in range(1, groups)
        ]

    def edges_begin():
        ends[0] = jnp.zeros(ends.shape[1:], jnp.float32)
        for slot in range(2):
            edges[0, parity(slot), 0:8, :] = mix[slot, rows - 8 : rows, :].astype(jnp.float32)
            edges[0, parity(slot), 8:16, :] = mix[slot, 0:8, :].astype(jnp.float32)
        for copy in swaps(edges, edge_send, edge_recv):
            copy.start()

    def edges_end():
        for copy in swaps(edges, edge_send, edge_recv):
            copy.wait_recv()
        for copy in swaps(edges, edge_send, edge_recv):
            copy.wait_send()

    def scan(layer, services):
        blocks = width // block
        chunk = rows // CHUNKS
        size = rows // ROW_STEPS
        pitch = chunk + 8

        def body(i, _):
            for when, m, kz in services:

                @pl.when(i == when)
                def _():
                    relay(m, kz)

            slot, b = div(i, blocks), rem(i, blocks)
            lanes = pl.ds(pl.multiple_of(b * block, 128), block)
            where = flip_bits(z, slot, nz) * ny + y
            even = rem(z + slot, 2)
            off, par = place_of(jnp.maximum(where - 1, 0))
            padded[0:8, :] = jnp.where(where > 0, edges[off, par, 0:8, lanes], 0.0)
            off, par = place_of(jnp.minimum(where + 1, nsp - 1))
            padded[rows + 8 : rows + 16, :] = jnp.where(
                where < nsp - 1, edges[off, par, 8:16, lanes], 0.0
            )
            padded[8 : rows + 8, :] = mix[slot, :, lanes].astype(jnp.float32)
            maps = jnp.concatenate([gates[layer, g, lanes, :] for g in range(4)], axis=1)
            maps = jnp.concatenate([maps, maps], axis=0)
            for step in range(ROW_STEPS):
                base = step * size
                conv = padded[base + 6 : base + 6 + size, :] * taps[layer, 0:1, lanes]
                for tap in range(1, 4):
                    conv += (
                        padded[base + 6 + tap : base + 6 + tap + size, :]
                        * taps[layer, tap : tap + 1, lanes]
                    )
                high = conv.astype(jnp.bfloat16)
                low = (conv - high.astype(jnp.float32)).astype(jnp.bfloat16)
                pre = jnp.dot(
                    jnp.concatenate([high, low], axis=1), maps, preferred_element_type=jnp.float32
                )
                for e, (decay_to, drive_to) in enumerate(((fa, fu), (ba, bu))):
                    pre_r = pre[:, 2 * e * block : (2 * e + 1) * block]
                    pre_i = pre[:, (2 * e + 1) * block : (2 * e + 2) * block]
                    speed = GATE_SCALE * rate[layer, e : e + 1, lanes]
                    fall = sigmoid(pre_r) * speed
                    series = jnp.full_like(fall, SERIES[-1])
                    for term in reversed(SERIES[:-1]):
                        series = series * fall + term
                    lost = fall * series
                    loss = lost * (2.0 - lost)
                    root = loss * lax.rsqrt(jnp.maximum(loss, 1e-30))
                    decay = 1.0 - lost
                    drive = root * sigmoid(pre_i) * conv
                    for c in range(base // chunk, (base + size) // chunk):
                        cut = slice(c * chunk - base, (c + 1) * chunk - base)
                        decay_to[c * pitch : c * pitch + chunk, :] = decay[cut]
                        drive_to[c * pitch : c * pitch + chunk, :] = drive[cut]

            def advance(j, carry):
                f_state, f_prod, b_state, b_prod = carry
                at = pl.ds(j, CHUNKS, stride=pitch)
                back = pl.ds(chunk - 1 - j, CHUNKS, stride=pitch)
                f_decay, b_decay = fa[at, :], ba[back, :]
                f_state = f_decay * f_state + fu[at, :]
                f_prod = f_decay * f_prod
                b_state = b_decay * b_state + bu[back, :]
                b_prod = b_decay * b_prod
                fh[at, :] = f_state
                fp[at, :] = f_prod
                bh[back, :] = b_state
                bp[back, :] = b_prod
                return f_state, f_prod, b_state, b_prod

            zeros = jnp.zeros((CHUNKS, block), jnp.float32)
            ones = jnp.ones((CHUNKS, block), jnp.float32)
            f_state, f_prod, b_state, b_prod = lax.fori_loop(
                0, chunk, advance, (zeros, ones, zeros, ones), unroll=8
            )
            f_in, b_in = [], [None] * CHUNKS
            state, prod = zeros[0:1], ones[0:1]
            for c in range(CHUNKS):
                f_in.append((state, prod))
                state = f_prod[c : c + 1] * state + f_state[c : c + 1]
                prod = f_prod[c : c + 1] * prod
            ends[0, even, 0:1, lanes] = prod
            ends[0, even, 1:2, lanes] = state
            state, prod = zeros[0:1], ones[0:1]
            for c in reversed(range(CHUNKS)):
                b_in[c] = (state, prod)
                state = b_prod[c : c + 1] * state + b_state[c : c + 1]
                prod = b_prod[c : c + 1] * prod
            ends[0, even, 2:3, lanes] = prod
            ends[0, even, 3:4, lanes] = state
            for c in range(CHUNKS):
                at = slice(c * chunk, (c + 1) * chunk)
                held = slice(c * pitch, c * pitch + chunk)
                f_local, b_local = fp[held, :], bp[held, :]
                both[slot, at, lanes] = (
                    fh[held, :] + f_local * f_in[c][0] + bh[held, :] + b_local * b_in[c][0]
                )
                cums[0, slot, at, lanes] = f_local * f_in[c][1]
                cums[1, slot, at, lanes] = b_local * b_in[c][1]
            return 0

        lax.fori_loop(0, 2 * blocks, body, 0)

    def exchange_ends():
        for copy in swaps(ends, end_send, end_recv):
            copy.start()
        for copy in swaps(ends, end_send, end_recv):
            copy.wait_recv()
        for copy in swaps(ends, end_send, end_recv):
            copy.wait_send()
        for slot in range(2):
            where = token_block(slot)
            forward = jnp.zeros((1, width), jnp.float32)
            backward = jnp.zeros((1, width), jnp.float32)
            for b in range(nsp - 1):
                off, par = place_of(jnp.int32(b))
                moved = ends[off, par, 0:1, :] * forward + ends[off, par, 1:2, :]
                forward = jnp.where(where > b, moved, forward)
            for b in range(nsp - 1, 0, -1):
                off, par = place_of(jnp.int32(b))
                moved = ends[off, par, 2:3, :] * backward + ends[off, par, 3:4, :]
                backward = jnp.where(where < b, moved, backward)
            states[slot, 0:1, :] = forward
            states[slot, 1:2, :] = backward

    def leave(layer, slot, order, relays, waits):
        step = 32
        m = 3 * layer + 2

        def finish(i, _):
            at = pl.ds(pl.multiple_of(i * step, step), step)
            total = both[slot, at, :] + cums[0, slot, at, :] * states[slot, 0:1, :]
            total = total + cums[1, slot, at, :] * states[slot, 1:2, :]
            gate = gate_z[slot, at, :].astype(jnp.float32)
            mixed[at, :] = (total * gate * sigmoid(gate)).astype(jnp.bfloat16)
            return 0

        lax.fori_loop(0, rows // step, finish, 0)

        def use(_, kz, ky):
            term = lax.dot_general(
                mixed[...], weights[m, kz * ny + ky], (((1,), (1,)), ((), ())),
                preferred_element_type=jnp.float32,
            )
            owner = owner_of(kz, ky)
            t = div(owner, per)
            far = rem(div(t, 2) + nx - x, nx)
            other = rem(t + core, 2)
            at = pl.ds(pl.multiple_of(rem(owner, per) * depth, 128), depth)
            part[slot, other, far, :, at] = term.astype(jnp.bfloat16)

        if waits:
            own_weight(m).wait()
        walk(all_steps((m,), order), relays, waits, use)

    def s_to_core(slot, k):
        return remote(
            part.at[slot, 1, k], core_in.at[slot, k], sc_send.at[slot, k], sc_recv.at[slot, k],
            core_peer,
        )

    def s_to_x(slot, k):
        return remote(
            part.at[slot, 0, k], x_in.at[slot, k - 1], sx_send.at[slot, k - 1],
            sx_recv.at[slot, k - 1], x_peer(k),
        )

    def s_to_z():
        return remote(part.at[1, 0, 0], z_in, sz_send.at[0], sz_recv.at[0], z_peer(1))

    def give(slot):
        for k in list(range(1, nx)) + [0]:
            s_to_core(slot, k).start()

    def tiles(body):
        step = 32

        def run(i, _):
            body(pl.ds(pl.multiple_of(i * step, step), step))
            return 0

        lax.fori_loop(0, rows // step, run, 0)

    def pass_on(slot):
        for k in range(1, nx):
            s_to_core(slot, k).wait_recv()

            def body(at):
                total = part[slot, 0, k, at, :].astype(jnp.float32)
                total = total + core_in[slot, k, at, :].astype(jnp.float32)
                part[slot, 0, k, at, :] = total.astype(jnp.bfloat16)

            tiles(body)
            s_to_x(slot, k).start()
        s_to_core(slot, 0).wait_recv()

    def summed(slot, at):
        total = part[slot, 0, 0, at, :].astype(jnp.float32)
        total = total + core_in[slot, 0, at, :].astype(jnp.float32)
        for k in range(1, nx):
            total = total + x_in[slot, k - 1, at, :].astype(jnp.float32)
        return total

    def land(slot):
        for k in range(1, nx):
            s_to_x(slot, k).wait_recv()

    def drain(slot):
        for k in range(nx):
            s_to_core(slot, k).wait_send()
        for k in range(1, nx):
            s_to_x(slot, k).wait_send()

    first_own = pltpu.make_async_copy(stream_ref, own, start_sem.at[0])
    first_feat = pltpu.make_async_copy(stream_ref, feats.at[0, column], start_sem.at[1])
    channel = pl.multiple_of(column * 2 * width + role * width, 128)
    small = [
        pltpu.make_async_copy(taps_hbm.at[:, :, pl.ds(channel, width)], taps, start_sem.at[2]),
        pltpu.make_async_copy(rate_hbm.at[:, :, pl.ds(channel, width)], rate, start_sem.at[3]),
        pltpu.make_async_copy(
            gates_hbm.at[:, :, pl.ds(pl.multiple_of(role * width, 128), width), :],
            gates, start_sem.at[4],
        ),
    ]
    first_own.start()
    first_feat.start()
    pl.semaphore_wait(barrier, len(peers))
    order = [k for k in range(2, nz)] + [1]
    far = order[:-1]
    send_own_weights((0,))
    send_weights((0, far[0]))
    f_to_z(stream_ref).start()
    gather_start(stream_ref)
    send_weights(*[(0, k) for k in far[1:]], (0, 1), (1, far[0]), (1, 1))
    send_weights(*[(1, k) for k in far[1:]])
    send_own_weights((1,))
    for m in range(3 * layers):
        own_weight(m).start()
    for copy in small:
        copy.start()
    send_weights(*[(2, k) for k in [far[0], 1] + far[1:]])
    send_own_weights((2,))

    for layer in range(layers):
        last = layer == layers - 1
        v, g, o = 3 * layer, 3 * layer + 1, 3 * layer + 2
        clear(layer)
        if layer == 0:
            gather_x(0)
            relay(v, far[0])
            gather_z()
            first_own.wait()
            first_feat.wait()
            gather_finish(0)
            normalize(layer, 0)
            for k in far[1:]:
                relay(v, k)
            gather_x(1)
            relay(v, 1)
            gather_finish(1)
            normalize(layer, 1)
            inward = [(v, kz, 0, None) for kz in [0] + order]
            inward += [(g, kz, 0, None) for kz in [0, far[0], 1] + far[1:]]
            inward += [
                (m, kz, ky, None) for m in (v, g) for kz in [0] + order for ky in range(1, ny)
            ]
            passing = [(g, k) for k in order]
            enter(layer, (0, 1), inward, passing, True)
        else:
            relay(g, nth(0))
            gather_x(0)

            @pl.when(role == 0)
            def _():
                for i in range(1, nz - 2):
                    relay(g, nth(i))

            gather_z()
            gather_finish(0)
            normalize(layer, 0)
            inward = all_steps((v,), [0] + order) + late_steps(g)
            middle = [(g, k) for k in range(2, nz - 1)]
            enter(layer, (0,), inward, [(g, nz - 1)], True, middle)
            relay(o, nth(0))
            gather_x(1)
            gather_finish(1)
            for i in range(1, nz - 2):
                relay(o, nth(i))
            normalize(layer, 1)
            enter(layer, (1,), inward, [], False)
        edges_begin()
        mixed_order = [far[0], 1] + far[1:]
        if layer == 0:
            for k in mixed_order:
                relay(o, k)
        edges_end()
        if layer == 0:
            for copy in small:
                copy.wait()
        if not last:
            send_weights((v + 3, 1))

            @pl.when(role == 1)
            def _():
                send_weights((v + 4, 1))

        scan(layer, [])
        exchange_ends()
        if layer != 0:
            relay(o, nth(nz - 2))
        if not last:
            send_weights(*[(v + 3, k) for k in far])

            @pl.when(role == 1)
            def _():
                send_weights(*[(v + 4, k) for k in reversed(far)])

            send_own_weights((v + 3, v + 4))
        leave(layer, 1, [0] + order, [], True)
        give(1)
        leave(layer, 0, [0] + order, [], False)
        pass_on(1)
        give(0)
        pass_on(0)
        if not last:
            relay(v + 3, 1)
        land(1)

        def send_over(at):
            part[1, 0, 0, at, :] = summed(1, at).astype(jnp.bfloat16)

        tiles(send_over)
        s_to_z().start()
        if not last:
            send_own_weights((v + 5,))
            relay(v + 3, far[0])
        land(0)
        if not last:
            for k in far[1:]:
                relay(v + 3, k)
        s_to_z().wait_recv()

        def renew(at):
            total = summed(0, at) + z_in[at, :].astype(jnp.float32)
            fresh = (own[at, :].astype(jnp.float32) + total).astype(jnp.bfloat16)
            own[at, :] = fresh
            if not last:
                feats[0, column, at, :] = fresh

        tiles(renew)
        if not last:
            f_to_z(own).start()
            gather_start(own)

            @pl.when(role == 0)
            def _():
                send_weights(*[(v + 4, k) for k in far], (v + 4, 1))
                send_weights(*[(v + 5, k) for k in far], (v + 5, 1))

            @pl.when(role == 1)
            def _():
                send_weights((v + 5, 1), *[(v + 5, k) for k in reversed(far)])

        drain(1)
        drain(0)
        s_to_z().wait_send()
    result = pltpu.make_async_copy(own, result_ref, out_sem.at[0])
    result.start()
    for m in range(3 * layers):
        for k in range(1, nz):
            z_weight(m, k).wait_send()
        for kz in range(nz):
            for ky in range(1, ny):
                y_weight(m, kz, ky, kz == 0).wait_send()
    result.wait()


def per_device(
    stream_in, norm_gain, value_proj, gate_proj, out_proj, conv_taps, block_gates, forget_rate
):
    nsp, ntp = lax.axis_size("sp"), lax.axis_size("tp")
    layers, depth, both_roles = value_proj.shape
    rows, size = stream_in.shape
    width = both_roles // 2
    block = block_gates.shape[-1]
    ny = 1 << ((nsp.bit_length() - 1) // 2)
    nz, nx, groups = nsp // ny, ntp // 2, nsp // 2
    maps = block_gates.reshape(layers, 4, both_roles, block)
    half, full = jnp.bfloat16, jnp.float32
    dma = pltpu.SemaphoreType.DMA
    slab = pltpu.VMEM((rows + 8 * CHUNKS, block), full)
    scratch = [
        pltpu.VMEM((2, ntp, rows, size), half),
        pltpu.VMEM((3 * layers, nsp, depth, width), half),
        pltpu.VMEM((rows, size), half),
        pltpu.VMEM((2, rows, width), half),
        pltpu.VMEM((2, rows, width), half),
        pltpu.VMEM((rows + 16, block), full),
        *[slab] * 8,
        pltpu.VMEM((2, rows, width), full),
        pltpu.VMEM((2, 2, rows, width), full),
        pltpu.VMEM((rows, width), half),
        pltpu.VMEM((2, 2, nx, rows, size), half),
        pltpu.VMEM((2, nx, rows, size), half),
        pltpu.VMEM((2, nx - 1, rows, size), half),
        pltpu.VMEM((rows, size), half),
        pltpu.VMEM((groups, 2, 16, width), full),
        pltpu.VMEM((groups, 2, 8, width), full),
        pltpu.VMEM((2, 8, width), full),
        pltpu.VMEM((layers, 4, width), full),
        pltpu.VMEM((layers, 4, width, block), half),
        pltpu.VMEM((layers, 2, width), full),
        dma((5,)),
        dma((3 * layers,)),
        dma((3 * layers, nz - 1)),
        dma((3 * layers, nz, ny - 1)),
        dma((3 * layers, nsp)),
        dma((1,)), dma((1,)), dma((2, nx - 1)), dma((2, nx - 1)), dma((2, nx)), dma((2, nx)),
        dma((1,)), dma((1,)), dma((2, nx - 1)), dma((2, nx - 1)), dma((2, nx)), dma((2, nx)),
        dma((groups - 1,)), dma((groups - 1,)), dma((groups - 1,)), dma((groups - 1,)),
        dma((1,)),
    ]
    anywhere = pl.BlockSpec(memory_space=pl.ANY)
    inside = pl.BlockSpec(memory_space=pltpu.VMEM)
    return pl.pallas_call(
        functools.partial(kernel, nsp, ntp, layers),
        out_shape=jax.ShapeDtypeStruct((rows, size), half),
        in_specs=[anywhere] * 4 + [inside] + [anywhere] * 3,
        out_specs=anywhere,
        scratch_shapes=scratch,
        compiler_params=pltpu.CompilerParams(
            collective_id=0, has_side_effects=True, vmem_limit_bytes=VMEM_BYTES
        ),
        name="layers",
    )(stream_in, value_proj, gate_proj, out_proj, norm_gain, conv_taps, maps, forget_rate)


def solution(mesh):
    placed = (
        P("sp", "tp"),
        P(),
        P(None, "sp", "tp"),
        P(None, "sp", "tp"),
        P(None, "sp", "tp"),
        P(),
        P(None, None, None, "tp", None),
        P(),
    )
    return jax.shard_map(
        per_device, mesh=mesh, in_specs=placed, out_specs=P("sp", "tp"), check_vma=False
    )
```

```python
import functools

import jax
import jax.numpy as jnp
from jax import lax
from jax.experimental import pallas as pl
from jax.experimental.pallas import tpu as pltpu
from jax.sharding import PartitionSpec as P

GATE_SCALE = 8.0
NORM_EPS = 1e-06
ROW_STEPS = 4
CHUNKS = 8
HALVES = 2
MESH = pl.DeviceIdType.MESH
VMEM_BYTES = 67043328
SERIES = (1.0, -1.0 / 2, 1.0 / 6, -1.0 / 24, 1.0 / 120, -1.0 / 720, 1.0 / 5040)


def rem(a, b):
    return lax.rem(a, jnp.int32(b))


def div(a, b):
    return lax.div(a, jnp.int32(b))


def flip_bits(a, b, count):
    total, bit = 0, 1
    while bit < count:
        total = total + bit * rem(div(a, bit) + (b // bit if isinstance(b, int) else div(b, bit)), 2)
        bit *= 2
    return total


def role_of(z):
    return rem(z + div(z, 2), 2)


def sigmoid(x):
    return 0.5 * jnp.tanh(0.5 * x) + 0.5


def kernel(
    nsp, ntp, layers,
    stream_ref, value_ref, gate_ref, back_ref, gain_ref, taps_hbm, gates_hbm, rate_hbm,
    result_ref,
    feats, weights, own, mix, gate_z, padded, fa, fu, ba, bu, fh, fp, bh, bp,
    both, cums, mixed, part, core_in, x_in, z_in, edges, ends, states, taps, gates, rate,
    start_sem, own_sem, wz_send, wy_send, w_recv,
    fz_send, fz_recv, fx_send, fx_recv, fc_send, fc_recv,
    sz_send, sz_recv, sx_send, sx_recv, sc_send, sc_recv,
    edge_send, edge_recv, end_send, end_recv, out_sem,
):
    ny = 1 << ((nsp.bit_length() - 1) // 2)
    nz, nx, groups, per = nsp // ny, ntp // 2, nsp // 2, nsp // ntp
    rank, column = lax.axis_index("sp"), lax.axis_index("tp")
    z, y, x, core = div(rank, ny), rem(rank, ny), div(column, 2), rem(column, 2)
    role = role_of(z)
    group = div(z, 2) * ny + y
    rows, width = mix.shape[1], mix.shape[2]
    depth = weights.shape[2]
    block = gates.shape[3]
    sources = (value_ref, gate_ref, back_ref)

    def z_peer(k):
        return (flip_bits(z, k, nz) * ny + y, column)

    def y_peer(k):
        return (z * ny + rem(y + k, ny), column)

    def x_peer(k):
        return (rank, rem(x + k, nx) * 2 + core)

    def group_peer(k):
        g = rem(group + k, groups)
        half = div(g, ny)
        return ((2 * half + rem(role + half, 2)) * ny + rem(g, ny), column)

    core_peer = (rank, x * 2 + 1 - core)
    peers = [z_peer(k) for k in range(1, nz)] + [y_peer(k) for k in range(1, ny)]
    peers += [x_peer(k) for k in range(1, nx)] + [core_peer]
    peers += [group_peer(k) for k in range(1, groups)]
    barrier = pltpu.get_barrier_semaphore()
    for peer in peers:
        pl.semaphore_signal(barrier, inc=1, device_id=peer, device_id_type=MESH)

    def remote(src, dst, send, recv, peer):
        return pltpu.make_async_remote_copy(
            src_ref=src, dst_ref=dst, send_sem=send, recv_sem=recv,
            device_id=peer, device_id_type=MESH,
        )

    def rows_of(m, which):
        return sources[m % 3].at[m // 3, :, pl.ds(pl.multiple_of(which * width, 128), width)]

    def own_weight(m):
        return pltpu.make_async_copy(rows_of(m, role), weights.at[m, 0], own_sem.at[m])

    def z_weight(m, k):
        there = role_of(flip_bits(z, k, nz))
        return remote(
            rows_of(m, there), weights.at[m, k * ny], wz_send.at[m, k - 1],
            w_recv.at[m, k * ny], z_peer(k),
        )

    def y_weight(m, kz, ky, first=False):
        src = rows_of(m, role) if first else weights.at[m, kz * ny]
        return remote(
            src, weights.at[m, kz * ny + ky], wy_send.at[m, kz, ky - 1],
            w_recv.at[m, kz * ny + ky], y_peer(ky),
        )

    def send_weights(*pairs):
        for m, k in pairs:
            z_weight(m, k).start()

    def send_own_weights(ms):
        for m in ms:
            for ky in range(1, ny):
                y_weight(m, 0, ky, True).start()

    def relay(m, kz):
        z_weight_wait(m, kz)
        for ky in range(1, ny):
            y_weight(m, kz, ky).start()

    def z_weight_wait(m, kz):
        remote(
            weights.at[m, kz * ny], weights.at[m, kz * ny], wz_send.at[m, 0],
            w_recv.at[m, kz * ny], core_peer,
        ).wait_recv()

    def y_weight_wait(m, p):
        remote(
            weights.at[m, p], weights.at[m, p], wz_send.at[m, 0], w_recv.at[m, p], core_peer
        ).wait_recv()

    split = rows // HALVES

    def cut(h):
        return pl.ds(h * split, split)

    def f_copy(src, slot, h, at_column, send, recv, peer):
        return remote(src.at[cut(h)], feats.at[slot, at_column, cut(h)], send, recv, peer)

    def column_of(k):
        return rem(x + nx - k, nx) * 2 + core

    def f_to_core(slot, k, h, src):
        return f_copy(
            src, slot, h, column_of(k), fc_send.at[slot, k, h], fc_recv.at[slot, k, h], core_peer
        )

    def f_to_x(slot, k, h, src):
        send, recv = fx_send.at[slot, k - 1, h], fx_recv.at[slot, k - 1, h]
        return f_copy(src, slot, h, column, send, recv, x_peer(k))

    def f_to_z(h, src):
        return f_copy(src, 1, h, column, fz_send.at[h], fz_recv.at[h], z_peer(1))

    def gather_start(h, src):
        for k in range(1, nx):
            f_to_x(0, k, h, src).start()
        f_to_core(0, 0, h, src).start()

    def gather_z(h):
        f_to_z(h, own).wait_recv()
        mine = feats.at[1, column]
        for k in range(1, nx):
            f_to_x(1, k, h, mine).start()
        f_to_core(1, 0, h, mine).start()

    def gather_x(slot, h):
        for k in range(1, nx):
            f_to_x(slot, k, h, own).wait_recv()
            f_to_core(slot, k, h, feats.at[slot, column_of(k)]).start()

    def gather_finish(slot, h):
        for k in range(nx):
            f_to_core(slot, k, h, feats.at[slot, column_of(k)]).wait_recv()
            f_to_core(slot, k, h, feats.at[slot, column_of(k)]).wait_send()
        for k in range(1, nx):
            f_to_x(slot, k, h, own).wait_send()
        if slot == 1:
            f_to_z(h, own).wait_send()

    def normalize(layer, slot, h):
        step = 16

        def body(i, _):
            at = pl.ds(pl.multiple_of(h * split + i * step, step), step)
            squares = None
            for t in range(ntp):
                values = feats[slot, t, at, :].astype(jnp.float32)
                total = jnp.sum(values * values, axis=1, keepdims=True)
                squares = total if squares is None else squares + total
            size = feats.shape[3]
            scale = lax.rsqrt(squares / (ntp * size) + NORM_EPS)
            for t in range(ntp):
                values = feats[slot, t, at, :].astype(jnp.float32)
                gain = gain_ref[layer : layer + 1, t * size : (t + 1) * size]
                feats[slot, t, at, :] = (values * scale * gain).astype(jnp.bfloat16)
            return 0

        lax.fori_loop(0, split // step, body, 0, unroll=2)

    def owner_of(kz, ky):
        return flip_bits(z, kz, nz) * ny + rem(y + ny - ky, ny)

    def table(j, values):
        found = jnp.int32(values[0])
        for i, value in enumerate(values):
            found = jnp.where(j == i, jnp.int32(value), found)
        return found

    def nth(i):
        return jnp.where(role == 1, jnp.int32(nz - 1 - i), jnp.int32(1 + i))

    def all_steps(ms, order):
        steps = [(m, kz, 0, None) for m in ms for kz in order]
        return steps + [(m, kz, ky, None) for m in ms for kz in order for ky in range(1, ny)]

    def late_steps(m):
        order = [(0, 0)] + [(k, nz - k) for k in range(1, nz)]
        steps = [(m, kz, 0, inner) for kz, inner in order]
        return steps + [(m, kz, ky, inner) for kz, inner in order for ky in range(1, ny)]

    def walk(steps, relays, waits, use, inner_relays=()):
        steps = [(m, kz, ky, kz if inner is None else inner) for m, kz, ky, inner in steps]
        columns = list(zip(*steps))
        passing = [int(ky == 0 and kz != 0 and (m, kz) in relays) for m, kz, ky, _ in steps]
        inside = [int(ky == 0 and kz != 0 and (m, kz) in inner_relays) for m, kz, ky, _ in steps]
        waiting = [int(waits and ky != 0) for _, _, ky, _ in steps]

        def body(j, _):
            m, outer, ky, inner = [table(j, column) for column in columns]
            kz = jnp.where(role == 1, inner, outer)

            if any(passing):

                @pl.when(table(j, passing) == 1)
                def _():
                    relay(m, kz)

            if any(waiting):

                @pl.when(table(j, waiting) == 1)
                def _():
                    y_weight_wait(m, kz * ny + ky)

            if any(inside):

                @pl.when(jnp.logical_and(role == 1, table(j, inside) == 1))
                def _():
                    relay(m, kz)

            use(m, kz, ky)
            return 0

        lax.fori_loop(0, len(steps), body, 0)

    def clear(layer):
        cums[...] = jnp.zeros_like(cums)
        for m in (3 * layer, 3 * layer + 1):
            own_weight(m).wait()

    def enter(layer, slots, steps, relays, waits, inner_relays=()):
        def use(m, kz, ky):
            owner = owner_of(kz, ky)
            t = div(owner, per)
            at = pl.ds(pl.multiple_of(rem(owner, per) * depth, 128), depth)
            for slot in slots:
                cums[m - 3 * layer, slot] += jnp.dot(
                    feats[slot, t, :, at], weights[m, kz * ny + ky],
                    preferred_element_type=jnp.float32,
                )

        walk(steps, relays, waits, use, inner_relays)
        for slot in slots:
            mix[slot] = cums[0, slot].astype(jnp.bfloat16)
            gate_z[slot] = cums[1, slot].astype(jnp.bfloat16)

    def parity(slot):
        return rem(z + slot, 2)

    def token_block(slot):
        return flip_bits(z, slot, nz) * ny + y

    def place_of(b):
        zb, yb = div(b, ny), rem(b, ny)
        there = div(zb, 2) * ny + yb
        return rem(group + groups - there, groups), rem(zb, 2)

    def swaps(cells, send, recv):
        return [
            remote(cells.at[0], cells.at[k], send.at[k - 1], recv.at[k - 1], group_peer(k))
            for k in range(1, groups)
        ]

    def edges_begin():
        ends[0] = jnp.zeros(ends.shape[1:], jnp.float32)
        for slot in range(2):
            edges[0, parity(slot), 0:8, :] = mix[slot, rows - 8 : rows, :].astype(jnp.float32)
            edges[0, parity(slot), 8:16, :] = mix[slot, 0:8, :].astype(jnp.float32)
        for copy in swaps(edges, edge_send, edge_recv):
            copy.start()

    def edges_end():
        for copy in swaps(edges, edge_send, edge_recv):
            copy.wait_recv()
        for copy in swaps(edges, edge_send, edge_recv):
            copy.wait_send()

    def scan(layer, services):
        blocks = width // block
        chunk = rows // CHUNKS
        size = rows // ROW_STEPS
        pitch = chunk + 8

        def body(i, _):
            for when, m, kz in services:

                @pl.when(i == when)
                def _():
                    relay(m, kz)

            slot, b = div(i, blocks), rem(i, blocks)
            lanes = pl.ds(pl.multiple_of(b * block, 128), block)
            where = flip_bits(z, slot, nz) * ny + y
            even = rem(z + slot, 2)
            off, par = place_of(jnp.maximum(where - 1, 0))
            padded[0:8, :] = jnp.where(where > 0, edges[off, par, 0:8, lanes], 0.0)
            off, par = place_of(jnp.minimum(where + 1, nsp - 1))
            padded[rows + 8 : rows + 16, :] = jnp.where(
                where < nsp - 1, edges[off, par, 8:16, lanes], 0.0
            )
            padded[8 : rows + 8, :] = mix[slot, :, lanes].astype(jnp.float32)
            maps = jnp.concatenate([gates[layer, g, lanes, :] for g in range(4)], axis=1)
            maps = jnp.concatenate([maps, maps], axis=0)
            for step in range(ROW_STEPS):
                base = step * size
                conv = padded[base + 6 : base + 6 + size, :] * taps[layer, 0:1, lanes]
                for tap in range(1, 4):
                    conv += (
                        padded[base + 6 + tap : base + 6 + tap + size, :]
                        * taps[layer, tap : tap + 1, lanes]
                    )
                high = conv.astype(jnp.bfloat16)
                low = (conv - high.astype(jnp.float32)).astype(jnp.bfloat16)
                pre = jnp.dot(
                    jnp.concatenate([high, low], axis=1), maps, preferred_element_type=jnp.float32
                )
                for e, (decay_to, drive_to) in enumerate(((fa, fu), (ba, bu))):
                    pre_r = pre[:, 2 * e * block : (2 * e + 1) * block]
                    pre_i = pre[:, (2 * e + 1) * block : (2 * e + 2) * block]
                    speed = GATE_SCALE * rate[layer, e : e + 1, lanes]
                    fall = sigmoid(pre_r) * speed
                    series = jnp.full_like(fall, SERIES[-1])
                    for term in reversed(SERIES[:-1]):
                        series = series * fall + term
                    lost = fall * series
                    loss = lost * (2.0 - lost)
                    root = loss * lax.rsqrt(jnp.maximum(loss, 1e-30))
                    decay = 1.0 - lost
                    drive = root * sigmoid(pre_i) * conv
                    for c in range(base // chunk, (base + size) // chunk):
                        cut = slice(c * chunk - base, (c + 1) * chunk - base)
                        decay_to[c * pitch : c * pitch + chunk, :] = decay[cut]
                        drive_to[c * pitch : c * pitch + chunk, :] = drive[cut]

            def advance(j, carry):
                f_state, f_prod, b_state, b_prod = carry
                at = pl.ds(j, CHUNKS, stride=pitch)
                back = pl.ds(chunk - 1 - j, CHUNKS, stride=pitch)
                f_decay, b_decay = fa[at, :], ba[back, :]
                f_state = f_decay * f_state + fu[at, :]
                f_prod = f_decay * f_prod
                b_state = b_decay * b_state + bu[back, :]
                b_prod = b_decay * b_prod
                fh[at, :] = f_state
                fp[at, :] = f_prod
                bh[back, :] = b_state
                bp[back, :] = b_prod
                return f_state, f_prod, b_state, b_prod

            zeros = jnp.zeros((CHUNKS, block), jnp.float32)
            ones = jnp.ones((CHUNKS, block), jnp.float32)
            f_state, f_prod, b_state, b_prod = lax.fori_loop(
                0, chunk, advance, (zeros, ones, zeros, ones), unroll=8
            )
            f_in, b_in = [], [None] * CHUNKS
            state, prod = zeros[0:1], ones[0:1]
            for c in range(CHUNKS):
                f_in.append((state, prod))
                state = f_prod[c : c + 1] * state + f_state[c : c + 1]
                prod = f_prod[c : c + 1] * prod
            ends[0, even, 0:1, lanes] = prod
            ends[0, even, 1:2, lanes] = state
            state, prod = zeros[0:1], ones[0:1]
            for c in reversed(range(CHUNKS)):
                b_in[c] = (state, prod)
                state = b_prod[c : c + 1] * state + b_state[c : c + 1]
                prod = b_prod[c : c + 1] * prod
            ends[0, even, 2:3, lanes] = prod
            ends[0, even, 3:4, lanes] = state
            for c in range(CHUNKS):
                at = slice(c * chunk, (c + 1) * chunk)
                held = slice(c * pitch, c * pitch + chunk)
                f_local, b_local = fp[held, :], bp[held, :]
                both[slot, at, lanes] = (
                    fh[held, :] + f_local * f_in[c][0] + bh[held, :] + b_local * b_in[c][0]
                )
                cums[0, slot, at, lanes] = f_local * f_in[c][1]
                cums[1, slot, at, lanes] = b_local * b_in[c][1]
            return 0

        lax.fori_loop(0, 2 * blocks, body, 0)

    def ends_begin():
        for copy in swaps(ends, end_send, end_recv):
            copy.start()

    def ends_end():
        for copy in swaps(ends, end_send, end_recv):
            copy.wait_recv()
        for copy in swaps(ends, end_send, end_recv):
            copy.wait_send()
        for slot in range(2):
            where = token_block(slot)
            forward = jnp.zeros((1, width), jnp.float32)
            backward = jnp.zeros((1, width), jnp.float32)
            for b in range(nsp - 1):
                off, par = place_of(jnp.int32(b))
                moved = ends[off, par, 0:1, :] * forward + ends[off, par, 1:2, :]
                forward = jnp.where(where > b, moved, forward)
            for b in range(nsp - 1, 0, -1):
                off, par = place_of(jnp.int32(b))
                moved = ends[off, par, 2:3, :] * backward + ends[off, par, 3:4, :]
                backward = jnp.where(where < b, moved, backward)
            states[slot, 0:1, :] = forward
            states[slot, 1:2, :] = backward

    def leave(layer, slot, order, relays, waits):
        step = 32
        m = 3 * layer + 2

        def finish(i, _):
            at = pl.ds(pl.multiple_of(i * step, step), step)
            total = both[slot, at, :] + cums[0, slot, at, :] * states[slot, 0:1, :]
            total = total + cums[1, slot, at, :] * states[slot, 1:2, :]
            gate = gate_z[slot, at, :].astype(jnp.float32)
            mixed[at, :] = (total * gate * sigmoid(gate)).astype(jnp.bfloat16)
            return 0

        lax.fori_loop(0, rows // step, finish, 0)

        def use(_, kz, ky):
            term = lax.dot_general(
                mixed[...], weights[m, kz * ny + ky], (((1,), (1,)), ((), ())),
                preferred_element_type=jnp.float32,
            )
            owner = owner_of(kz, ky)
            t = div(owner, per)
            far = rem(div(t, 2) + nx - x, nx)
            other = rem(t + core, 2)
            at = pl.ds(pl.multiple_of(rem(owner, per) * depth, 128), depth)
            part[slot, other, far, :, at] = term.astype(jnp.bfloat16)

        if waits:
            own_weight(m).wait()
        walk(all_steps((m,), order), relays, waits, use)

    def s_to_core(slot, k, h):
        return remote(
            part.at[slot, 1, k, cut(h)], core_in.at[slot, k, cut(h)],
            sc_send.at[slot, k, h], sc_recv.at[slot, k, h], core_peer,
        )

    def s_to_x(slot, k, h):
        return remote(
            part.at[slot, 0, k, cut(h)], x_in.at[slot, k - 1, cut(h)],
            sx_send.at[slot, k - 1, h], sx_recv.at[slot, k - 1, h], x_peer(k),
        )

    def s_to_z(h, k=0):
        there = z_in.at[cut(h)] if k == 0 else x_in.at[1, k - 1, cut(h)]
        index = h if k == 0 else HALVES + k - 1
        return remote(
            part.at[1, 0, k, cut(h)], there, sz_send.at[index], sz_recv.at[index], z_peer(1)
        )

    def give(slot):
        for h in range(HALVES):
            for k in list(range(1, nx)) + [0]:
                s_to_core(slot, k, h).start()

    def tiles(h, body):
        step = 32

        def run(i, _):
            body(pl.ds(pl.multiple_of(h * split + i * step, step), step))
            return 0

        lax.fori_loop(0, split // step, run, 0)

    def add_core(slot, k, h, more=None):
        def body(at):
            total = part[slot, 0, k, at, :].astype(jnp.float32)
            total = total + core_in[slot, k, at, :].astype(jnp.float32)
            if more is not None:
                total = total + more[at, :].astype(jnp.float32)
            part[slot, 0, k, at, :] = total.astype(jnp.bfloat16)

        tiles(h, body)

    def pass_on(slot, h):
        for k in range(1, nx):
            s_to_core(slot, k, h).wait_recv()
            add_core(slot, k, h)
            s_to_x(slot, k, h).start()
        s_to_core(slot, 0, h).wait_recv()

    def pass_over(h):
        for k in list(range(1, nx)) + [0]:
            s_to_core(1, k, h).wait_recv()
            add_core(1, k, h)
            s_to_z(h, k).start()

    def pass_joined(h):
        for k in range(1, nx):
            s_to_core(0, k, h).wait_recv()
            s_to_z(h, k).wait_recv()
            add_core(0, k, h, x_in.at[1, k - 1])
            s_to_x(0, k, h).start()
        s_to_core(0, 0, h).wait_recv()

    def summed(slot, at):
        total = part[slot, 0, 0, at, :].astype(jnp.float32)
        total = total + core_in[slot, 0, at, :].astype(jnp.float32)
        for k in range(1, nx):
            total = total + x_in[slot, k - 1, at, :].astype(jnp.float32)
        return total

    def land(slot, h):
        for k in range(1, nx):
            s_to_x(slot, k, h).wait_recv()

    def send_over(h):
        land(1, h)

        def body(at):
            part[1, 0, 0, at, :] = summed(1, at).astype(jnp.bfloat16)

        tiles(h, body)
        s_to_z(h).start()

    def renew(h, last):
        land(0, h)
        s_to_z(h).wait_recv()

        def body(at):
            total = summed(0, at) + z_in[at, :].astype(jnp.float32)
            fresh = (own[at, :].astype(jnp.float32) + total).astype(jnp.bfloat16)
            own[at, :] = fresh
            if not last:
                feats[0, column, at, :] = fresh

        tiles(h, body)

    def drain(crossed):
        for h in range(HALVES):
            for slot in range(2):
                for k in range(nx):
                    s_to_core(slot, k, h).wait_send()
                for k in range(1, nx):
                    if slot == 0 or h not in crossed:
                        s_to_x(slot, k, h).wait_send()
            s_to_z(h).wait_send()
            for k in range(1, nx):
                if h in crossed:
                    s_to_z(h, k).wait_send()

    first_own = pltpu.make_async_copy(stream_ref, own, start_sem.at[0])
    first_feat = pltpu.make_async_copy(stream_ref, feats.at[0, column], start_sem.at[1])
    channel = pl.multiple_of(column * 2 * width + role * width, 128)
    small = [
        pltpu.make_async_copy(taps_hbm.at[:, :, pl.ds(channel, width)], taps, start_sem.at[2]),
        pltpu.make_async_copy(rate_hbm.at[:, :, pl.ds(channel, width)], rate, start_sem.at[3]),
        pltpu.make_async_copy(
            gates_hbm.at[:, :, pl.ds(pl.multiple_of(role * width, 128), width), :],
            gates, start_sem.at[4],
        ),
    ]
    first_own.start()
    first_feat.start()
    pl.semaphore_wait(barrier, len(peers))
    order = [k for k in range(2, nz)] + [1]
    far = order[:-1]
    halves = range(HALVES)
    send_own_weights((0, 1))
    send_weights((0, far[0]))
    for h in halves:
        f_to_z(h, stream_ref).start()
        gather_start(h, stream_ref)
    send_weights(*[(0, k) for k in far[1:]], (0, 1), (1, far[0]), (1, 1))
    send_weights(*[(1, k) for k in far[1:]], (2, far[0]), (2, 1))
    for m in range(3 * layers):
        own_weight(m).start()
    for copy in small:
        copy.start()
    send_own_weights((2,))
    results = []

    for layer in range(layers):
        last = layer == layers - 1
        v, g, o = 3 * layer, 3 * layer + 1, 3 * layer + 2
        clear(layer)
        if layer == 0:
            gather_x(0, 0)
            relay(v, far[0])
            for h in range(1, HALVES):
                gather_x(0, h)
            for k in far[1:]:
                relay(v, k)
            for h in halves:
                gather_z(h)
            relay(v, 1)
            first_own.wait()
            first_feat.wait()
            for h in halves:
                gather_finish(0, h)
                normalize(layer, 0, h)
            relay(g, far[0])
            for h in halves:
                gather_x(1, h)
            relay(g, 1)
            for h in halves:
                gather_finish(1, h)
                normalize(layer, 1, h)
            inward = all_steps((v,), [0] + order)
            inward += all_steps((g,), [0, far[0], 1] + far[1:])
            enter(layer, (0, 1), inward, [(g, k) for k in far[1:]], True)
        else:
            relay(g, nth(0))
            for h in halves:
                gather_x(0, h)
                gather_z(h)

            @pl.when(role == 0)
            def _():
                for i in range(1, nz - 2):
                    relay(g, nth(i))

            @pl.when(role == 1)
            def _():
                send_weights((o, 1), *[(o, k) for k in reversed(far)])

            for h in halves:
                gather_finish(0, h)
                normalize(layer, 0, h)
            inward = all_steps((v,), [0] + order) + late_steps(g)
            middle = [(g, k) for k in range(2, nz - 1)]
            enter(layer, (0,), inward, [(g, nz - 1)], True, middle)
            relay(o, nth(0))
            for h in halves:
                gather_x(1, h)
            for h in halves:
                gather_finish(1, h)
                normalize(layer, 1, h)
            enter(layer, (1,), inward, [], False)
        edges_begin()
        if layer == 0:
            send_weights(*[(o, k) for k in far[1:]])
            relay(o, far[0])
            relay(o, 1)
        else:
            for i in range(1, nz - 2):
                relay(o, nth(i))
        edges_end()
        if layer == 0:
            for copy in small:
                copy.wait()
        if not last:
            send_weights((v + 3, 1))

            @pl.when(role == 1)
            def _():
                send_weights((v + 4, 1))

        scan(layer, [])
        ends_begin()
        if layer == 0:
            for k in far[1:]:
                relay(o, k)
        ends_end()
        if layer != 0:
            relay(o, nth(nz - 2))
        if not last:
            send_weights(*[(v + 3, k) for k in far])

            @pl.when(role == 1)
            def _():
                send_weights(*[(v + 4, k) for k in reversed(far)])

            send_own_weights((v + 3, v + 4))
        leave(layer, 1, [0] + order, [], True)
        give(1)
        crossed = [h for h in halves if last and h >= (HALVES + 1) // 2]
        for h in halves:
            if h in crossed:
                pass_over(h)
            else:
                pass_on(1, h)
        leave(layer, 0, [0] + order, [], False)
        give(0)
        for h in halves:
            if h in crossed:
                pass_joined(h)
            else:
                pass_on(0, h)
        if not last:
            relay(v + 3, 1)
        for h in halves:
            if h not in crossed:
                send_over(h)
        if not last:

            @pl.when(role == 0)
            def _():
                send_weights((v + 4, far[0]))

            send_own_weights((v + 5,))
            relay(v + 3, far[0])
        for h in halves:
            renew(h, last)
            if not last:
                f_to_z(h, own).start()
                gather_start(h, own)
            else:
                result = pltpu.make_async_copy(
                    own.at[cut(h)], result_ref.at[cut(h)], out_sem.at[h]
                )
                result.start()
                results.append(result)
        if not last:
            for k in far[1:]:
                relay(v + 3, k)

            @pl.when(role == 0)
            def _():
                send_weights(*[(v + 4, k) for k in far[1:]], (v + 4, 1))
                send_weights(*[(v + 5, k) for k in far], (v + 5, 1))

        drain(crossed)
    for m in range(3 * layers):
        for k in range(1, nz):
            z_weight(m, k).wait_send()
        for kz in range(nz):
            for ky in range(1, ny):
                y_weight(m, kz, ky, kz == 0).wait_send()
    for result in results:
        result.wait()


def per_device(
    stream_in, norm_gain, value_proj, gate_proj, out_proj, conv_taps, block_gates, forget_rate
):
    nsp, ntp = lax.axis_size("sp"), lax.axis_size("tp")
    layers, depth, both_roles = value_proj.shape
    rows, size = stream_in.shape
    width = both_roles // 2
    block = block_gates.shape[-1]
    ny = 1 << ((nsp.bit_length() - 1) // 2)
    nz, nx, groups = nsp // ny, ntp // 2, nsp // 2
    maps = block_gates.reshape(layers, 4, both_roles, block)
    half, full = jnp.bfloat16, jnp.float32
    dma = pltpu.SemaphoreType.DMA
    slab = pltpu.VMEM((rows + 8 * CHUNKS, block), full)
    scratch = [
        pltpu.VMEM((2, ntp, rows, size), half),
        pltpu.VMEM((3 * layers, nsp, depth, width), half),
        pltpu.VMEM((rows, size), half),
        pltpu.VMEM((2, rows, width), half),
        pltpu.VMEM((2, rows, width), half),
        pltpu.VMEM((rows + 16, block), full),
        *[slab] * 8,
        pltpu.VMEM((2, rows, width), full),
        pltpu.VMEM((2, 2, rows, width), full),
        pltpu.VMEM((rows, width), half),
        pltpu.VMEM((2, 2, nx, rows, size), half),
        pltpu.VMEM((2, nx, rows, size), half),
        pltpu.VMEM((2, nx - 1, rows, size), half),
        pltpu.VMEM((rows, size), half),
        pltpu.VMEM((groups, 2, 16, width), full),
        pltpu.VMEM((groups, 2, 8, width), full),
        pltpu.VMEM((2, 8, width), full),
        pltpu.VMEM((layers, 4, width), full),
        pltpu.VMEM((layers, 4, width, block), half),
        pltpu.VMEM((layers, 2, width), full),
        dma((5,)),
        dma((3 * layers,)),
        dma((3 * layers, nz - 1)),
        dma((3 * layers, nz, ny - 1)),
        dma((3 * layers, nsp)),
        dma((HALVES,)), dma((HALVES,)),
        *[dma((2, nx - 1, HALVES))] * 2, *[dma((2, nx, HALVES))] * 2,
        dma((HALVES + nx - 1,)), dma((HALVES + nx - 1,)),
        *[dma((2, nx - 1, HALVES))] * 2, *[dma((2, nx, HALVES))] * 2,
        dma((groups - 1,)), dma((groups - 1,)), dma((groups - 1,)), dma((groups - 1,)),
        dma((HALVES,)),
    ]
    anywhere = pl.BlockSpec(memory_space=pl.ANY)
    inside = pl.BlockSpec(memory_space=pltpu.VMEM)
    return pl.pallas_call(
        functools.partial(kernel, nsp, ntp, layers),
        out_shape=jax.ShapeDtypeStruct((rows, size), half),
        in_specs=[anywhere] * 4 + [inside] + [anywhere] * 3,
        out_specs=anywhere,
        scratch_shapes=scratch,
        compiler_params=pltpu.CompilerParams(
            collective_id=0, has_side_effects=True, vmem_limit_bytes=VMEM_BYTES
        ),
        name="layers",
    )(stream_in, value_proj, gate_proj, out_proj, norm_gain, conv_taps, maps, forget_rate)


def solution(mesh):
    placed = (
        P("sp", "tp"),
        P(),
        P(None, "sp", "tp"),
        P(None, "sp", "tp"),
        P(None, "sp", "tp"),
        P(),
        P(None, None, None, "tp", None),
        P(),
    )
    return jax.shard_map(
        per_device, mesh=mesh, in_specs=placed, out_specs=P("sp", "tp"), check_vma=False
    )
```

```python
import functools

import jax
import jax.numpy as jnp
from jax import lax
from jax.experimental import pallas as pl
from jax.experimental.pallas import tpu as pltpu
from jax.sharding import PartitionSpec as P

GATE_SCALE = 8.0
NORM_EPS = 1e-06
ROW_STEPS = 4
CHUNKS = 8
HALVES = 4
MESH = pl.DeviceIdType.MESH
VMEM_BYTES = 67043328
SERIES = (1.0, -1.0 / 2, 1.0 / 6, -1.0 / 24, 1.0 / 120, -1.0 / 720, 1.0 / 5040)


def rem(a, b):
    return lax.rem(a, jnp.int32(b))


def div(a, b):
    return lax.div(a, jnp.int32(b))


def flip_bits(a, b, count):
    total, bit = 0, 1
    while bit < count:
        total = total + bit * rem(div(a, bit) + (b // bit if isinstance(b, int) else div(b, bit)), 2)
        bit *= 2
    return total


def role_of(z):
    return rem(z + div(z, 2), 2)


def sigmoid(x):
    return 0.5 * jnp.tanh(0.5 * x) + 0.5


def kernel(
    nsp, ntp, layers,
    stream_ref, value_ref, gate_ref, back_ref, gain_ref, taps_hbm, gates_hbm, rate_hbm,
    result_ref,
    feats, weights, own, mix, gate_z, padded, fa, fu, ba, bu, fh, fp, bh, bp,
    both, cums, mixed, part, core_in, x_in, z_in, edges, ends, states, taps, gates, rate,
    start_sem, own_sem, wz_send, wy_send, w_recv,
    fz_send, fz_recv, fx_send, fx_recv, fc_send, fc_recv,
    sz_send, sz_recv, sx_send, sx_recv, sc_send, sc_recv,
    edge_send, edge_recv, end_send, end_recv, out_sem,
):
    ny = 1 << ((nsp.bit_length() - 1) // 2)
    nz, nx, groups, per = nsp // ny, ntp // 2, nsp // 2, nsp // ntp
    rank, column = lax.axis_index("sp"), lax.axis_index("tp")
    z, y, x, core = div(rank, ny), rem(rank, ny), div(column, 2), rem(column, 2)
    role = role_of(z)
    group = div(z, 2) * ny + y
    rows, width = mix.shape[1], mix.shape[2]
    depth = weights.shape[2]
    block = gates.shape[3]
    sources = (value_ref, gate_ref, back_ref)

    def z_peer(k):
        return (flip_bits(z, k, nz) * ny + y, column)

    def y_peer(k):
        return (z * ny + rem(y + k, ny), column)

    def x_peer(k):
        return (rank, rem(x + k, nx) * 2 + core)

    def group_peer(k):
        g = rem(group + k, groups)
        half = div(g, ny)
        return ((2 * half + rem(role + half, 2)) * ny + rem(g, ny), column)

    core_peer = (rank, x * 2 + 1 - core)
    peers = [z_peer(k) for k in range(1, nz)] + [y_peer(k) for k in range(1, ny)]
    peers += [x_peer(k) for k in range(1, nx)] + [core_peer]
    peers += [group_peer(k) for k in range(1, groups)]
    barrier = pltpu.get_barrier_semaphore()
    for peer in peers:
        pl.semaphore_signal(barrier, inc=1, device_id=peer, device_id_type=MESH)

    def remote(src, dst, send, recv, peer):
        return pltpu.make_async_remote_copy(
            src_ref=src, dst_ref=dst, send_sem=send, recv_sem=recv,
            device_id=peer, device_id_type=MESH,
        )

    def rows_of(m, which):
        return sources[m % 3].at[m // 3, :, pl.ds(pl.multiple_of(which * width, 128), width)]

    def own_weight(m):
        return pltpu.make_async_copy(rows_of(m, role), weights.at[m, 0], own_sem.at[m])

    def z_weight(m, k):
        there = role_of(flip_bits(z, k, nz))
        return remote(
            rows_of(m, there), weights.at[m, k * ny], wz_send.at[m, k - 1],
            w_recv.at[m, k * ny], z_peer(k),
        )

    def y_weight(m, kz, ky, first=False):
        src = rows_of(m, role) if first else weights.at[m, kz * ny]
        return remote(
            src, weights.at[m, kz * ny + ky], wy_send.at[m, kz, ky - 1],
            w_recv.at[m, kz * ny + ky], y_peer(ky),
        )

    def send_weights(*pairs):
        for m, k in pairs:
            z_weight(m, k).start()

    def send_own_weights(ms):
        for m in ms:
            for ky in range(1, ny):
                y_weight(m, 0, ky, True).start()

    def relay(m, kz):
        z_weight_wait(m, kz)
        for ky in range(1, ny):
            y_weight(m, kz, ky).start()

    def z_weight_wait(m, kz):
        remote(
            weights.at[m, kz * ny], weights.at[m, kz * ny], wz_send.at[m, 0],
            w_recv.at[m, kz * ny], core_peer,
        ).wait_recv()

    def y_weight_wait(m, p):
        remote(
            weights.at[m, p], weights.at[m, p], wz_send.at[m, 0], w_recv.at[m, p], core_peer
        ).wait_recv()

    split = rows // HALVES

    def cut(h):
        return pl.ds(h * split, split)

    def f_copy(src, slot, h, at_column, send, recv, peer):
        return remote(src.at[cut(h)], feats.at[slot, at_column, cut(h)], send, recv, peer)

    def column_of(k):
        return rem(x + nx - k, nx) * 2 + core

    def f_to_core(slot, k, h, src):
        return f_copy(
            src, slot, h, column_of(k), fc_send.at[slot, k, h], fc_recv.at[slot, k, h], core_peer
        )

    def f_to_x(slot, k, h, src):
        send, recv = fx_send.at[slot, k - 1, h], fx_recv.at[slot, k - 1, h]
        return f_copy(src, slot, h, column, send, recv, x_peer(k))

    def f_to_z(h, src):
        return f_copy(src, 1, h, column, fz_send.at[h], fz_recv.at[h], z_peer(1))

    def gather_start(h, src):
        for k in range(1, nx):
            f_to_x(0, k, h, src).start()
        f_to_core(0, 0, h, src).start()

    def gather_z(h):
        f_to_z(h, own).wait_recv()
        mine = feats.at[1, column]
        for k in range(1, nx):
            f_to_x(1, k, h, mine).start()
        f_to_core(1, 0, h, mine).start()

    def gather_x(slot, h):
        for k in range(1, nx):
            f_to_x(slot, k, h, own).wait_recv()
            f_to_core(slot, k, h, feats.at[slot, column_of(k)]).start()

    def gather_finish(slot, h):
        for k in range(nx):
            f_to_core(slot, k, h, feats.at[slot, column_of(k)]).wait_recv()
            f_to_core(slot, k, h, feats.at[slot, column_of(k)]).wait_send()
        for k in range(1, nx):
            f_to_x(slot, k, h, own).wait_send()
        if slot == 1:
            f_to_z(h, own).wait_send()

    def normalize(layer, slot, h):
        step = 16

        def body(i, _):
            at = pl.ds(pl.multiple_of(h * split + i * step, step), step)
            squares = None
            for t in range(ntp):
                values = feats[slot, t, at, :].astype(jnp.float32)
                total = jnp.sum(values * values, axis=1, keepdims=True)
                squares = total if squares is None else squares + total
            size = feats.shape[3]
            scale = lax.rsqrt(squares / (ntp * size) + NORM_EPS)
            for t in range(ntp):
                values = feats[slot, t, at, :].astype(jnp.float32)
                gain = gain_ref[layer : layer + 1, t * size : (t + 1) * size]
                feats[slot, t, at, :] = (values * scale * gain).astype(jnp.bfloat16)
            return 0

        lax.fori_loop(0, split // step, body, 0, unroll=2)

    def owner_of(kz, ky):
        return flip_bits(z, kz, nz) * ny + rem(y + ny - ky, ny)

    def table(j, values):
        found = jnp.int32(values[0])
        for i, value in enumerate(values):
            found = jnp.where(j == i, jnp.int32(value), found)
        return found

    def nth(i):
        return jnp.where(role == 1, jnp.int32(nz - 1 - i), jnp.int32(1 + i))

    def all_steps(ms, order):
        steps = [(m, kz, 0, None) for m in ms for kz in order]
        return steps + [(m, kz, ky, None) for m in ms for kz in order for ky in range(1, ny)]

    def late_steps(m):
        order = [(0, 0)] + [(k, nz - k) for k in range(1, nz)]
        steps = [(m, kz, 0, inner) for kz, inner in order]
        return steps + [(m, kz, ky, inner) for kz, inner in order for ky in range(1, ny)]

    def walk(steps, relays, waits, use, inner_relays=()):
        steps = [(m, kz, ky, kz if inner is None else inner) for m, kz, ky, inner in steps]
        columns = list(zip(*steps))
        passing = [int(ky == 0 and kz != 0 and (m, kz) in relays) for m, kz, ky, _ in steps]
        inside = [int(ky == 0 and kz != 0 and (m, kz) in inner_relays) for m, kz, ky, _ in steps]
        waiting = [int(waits and ky != 0) for _, _, ky, _ in steps]

        def body(j, _):
            m, outer, ky, inner = [table(j, column) for column in columns]
            kz = jnp.where(role == 1, inner, outer)

            if any(passing):

                @pl.when(table(j, passing) == 1)
                def _():
                    relay(m, kz)

            if any(waiting):

                @pl.when(table(j, waiting) == 1)
                def _():
                    y_weight_wait(m, kz * ny + ky)

            if any(inside):

                @pl.when(jnp.logical_and(role == 1, table(j, inside) == 1))
                def _():
                    relay(m, kz)

            use(m, kz, ky)
            return 0

        lax.fori_loop(0, len(steps), body, 0)

    def clear(layer):
        cums[...] = jnp.zeros_like(cums)
        for m in (3 * layer, 3 * layer + 1):
            own_weight(m).wait()

    def enter(layer, slots, steps, relays, waits, inner_relays=()):
        def use(m, kz, ky):
            owner = owner_of(kz, ky)
            t = div(owner, per)
            at = pl.ds(pl.multiple_of(rem(owner, per) * depth, 128), depth)
            for slot in slots:
                cums[m - 3 * layer, slot] += jnp.dot(
                    feats[slot, t, :, at], weights[m, kz * ny + ky],
                    preferred_element_type=jnp.float32,
                )

        walk(steps, relays, waits, use, inner_relays)
        for slot in slots:
            mix[slot] = cums[0, slot].astype(jnp.bfloat16)
            gate_z[slot] = cums[1, slot].astype(jnp.bfloat16)

    def parity(slot):
        return rem(z + slot, 2)

    def token_block(slot):
        return flip_bits(z, slot, nz) * ny + y

    def place_of(b):
        zb, yb = div(b, ny), rem(b, ny)
        there = div(zb, 2) * ny + yb
        return rem(group + groups - there, groups), rem(zb, 2)

    def swaps(cells, send, recv):
        return [
            remote(cells.at[0], cells.at[k], send.at[k - 1], recv.at[k - 1], group_peer(k))
            for k in range(1, groups)
        ]

    def edges_begin():
        ends[0] = jnp.zeros(ends.shape[1:], jnp.float32)
        for slot in range(2):
            edges[0, parity(slot), 0:8, :] = mix[slot, rows - 8 : rows, :].astype(jnp.float32)
            edges[0, parity(slot), 8:16, :] = mix[slot, 0:8, :].astype(jnp.float32)
        for copy in swaps(edges, edge_send, edge_recv):
            copy.start()

    def edges_end():
        for copy in swaps(edges, edge_send, edge_recv):
            copy.wait_recv()
        for copy in swaps(edges, edge_send, edge_recv):
            copy.wait_send()

    def scan(layer, services):
        blocks = width // block
        chunk = rows // CHUNKS
        size = rows // ROW_STEPS
        pitch = chunk + 8

        def body(i, _):
            for when, m, kz in services:

                @pl.when(i == when)
                def _():
                    relay(m, kz)

            slot, b = div(i, blocks), rem(i, blocks)
            lanes = pl.ds(pl.multiple_of(b * block, 128), block)
            where = flip_bits(z, slot, nz) * ny + y
            even = rem(z + slot, 2)
            off, par = place_of(jnp.maximum(where - 1, 0))
            padded[0:8, :] = jnp.where(where > 0, edges[off, par, 0:8, lanes], 0.0)
            off, par = place_of(jnp.minimum(where + 1, nsp - 1))
            padded[rows + 8 : rows + 16, :] = jnp.where(
                where < nsp - 1, edges[off, par, 8:16, lanes], 0.0
            )
            padded[8 : rows + 8, :] = mix[slot, :, lanes].astype(jnp.float32)
            maps = jnp.concatenate([gates[layer, g, lanes, :] for g in range(4)], axis=1)
            maps = jnp.concatenate([maps, maps], axis=0)
            for step in range(ROW_STEPS):
                base = step * size
                conv = padded[base + 6 : base + 6 + size, :] * taps[layer, 0:1, lanes]
                for tap in range(1, 4):
                    conv += (
                        padded[base + 6 + tap : base + 6 + tap + size, :]
                        * taps[layer, tap : tap + 1, lanes]
                    )
                high = conv.astype(jnp.bfloat16)
                low = (conv - high.astype(jnp.float32)).astype(jnp.bfloat16)
                pre = jnp.dot(
                    jnp.concatenate([high, low], axis=1), maps, preferred_element_type=jnp.float32
                )
                for e, (decay_to, drive_to) in enumerate(((fa, fu), (ba, bu))):
                    pre_r = pre[:, 2 * e * block : (2 * e + 1) * block]
                    pre_i = pre[:, (2 * e + 1) * block : (2 * e + 2) * block]
                    speed = GATE_SCALE * rate[layer, e : e + 1, lanes]
                    fall = sigmoid(pre_r) * speed
                    series = jnp.full_like(fall, SERIES[-1])
                    for term in reversed(SERIES[:-1]):
                        series = series * fall + term
                    lost = fall * series
                    loss = lost * (2.0 - lost)
                    root = loss * lax.rsqrt(jnp.maximum(loss, 1e-30))
                    decay = 1.0 - lost
                    drive = root * sigmoid(pre_i) * conv
                    for c in range(base // chunk, (base + size) // chunk):
                        cut = slice(c * chunk - base, (c + 1) * chunk - base)
                        decay_to[c * pitch : c * pitch + chunk, :] = decay[cut]
                        drive_to[c * pitch : c * pitch + chunk, :] = drive[cut]

            def advance(j, carry):
                f_state, f_prod, b_state, b_prod = carry
                at = pl.ds(j, CHUNKS, stride=pitch)
                back = pl.ds(chunk - 1 - j, CHUNKS, stride=pitch)
                f_decay, b_decay = fa[at, :], ba[back, :]
                f_state = f_decay * f_state + fu[at, :]
                f_prod = f_decay * f_prod
                b_state = b_decay * b_state + bu[back, :]
                b_prod = b_decay * b_prod
                fh[at, :] = f_state
                fp[at, :] = f_prod
                bh[back, :] = b_state
                bp[back, :] = b_prod
                return f_state, f_prod, b_state, b_prod

            zeros = jnp.zeros((CHUNKS, block), jnp.float32)
            ones = jnp.ones((CHUNKS, block), jnp.float32)
            f_state, f_prod, b_state, b_prod = lax.fori_loop(
                0, chunk, advance, (zeros, ones, zeros, ones), unroll=8
            )
            f_in, b_in = [], [None] * CHUNKS
            state, prod = zeros[0:1], ones[0:1]
            for c in range(CHUNKS):
                f_in.append((state, prod))
                state = f_prod[c : c + 1] * state + f_state[c : c + 1]
                prod = f_prod[c : c + 1] * prod
            ends[0, even, 0:1, lanes] = prod
            ends[0, even, 1:2, lanes] = state
            state, prod = zeros[0:1], ones[0:1]
            for c in reversed(range(CHUNKS)):
                b_in[c] = (state, prod)
                state = b_prod[c : c + 1] * state + b_state[c : c + 1]
                prod = b_prod[c : c + 1] * prod
            ends[0, even, 2:3, lanes] = prod
            ends[0, even, 3:4, lanes] = state
            for c in range(CHUNKS):
                at = slice(c * chunk, (c + 1) * chunk)
                held = slice(c * pitch, c * pitch + chunk)
                f_local, b_local = fp[held, :], bp[held, :]
                both[slot, at, lanes] = (
                    fh[held, :] + f_local * f_in[c][0] + bh[held, :] + b_local * b_in[c][0]
                )
                cums[0, slot, at, lanes] = f_local * f_in[c][1]
                cums[1, slot, at, lanes] = b_local * b_in[c][1]
            return 0

        lax.fori_loop(0, 2 * blocks, body, 0)

    def ends_begin():
        for copy in swaps(ends, end_send, end_recv):
            copy.start()

    def ends_end():
        for copy in swaps(ends, end_send, end_recv):
            copy.wait_recv()
        for copy in swaps(ends, end_send, end_recv):
            copy.wait_send()
        for slot in range(2):
            where = token_block(slot)
            forward = jnp.zeros((1, width), jnp.float32)
            backward = jnp.zeros((1, width), jnp.float32)
            for b in range(nsp - 1):
                off, par = place_of(jnp.int32(b))
                moved = ends[off, par, 0:1, :] * forward + ends[off, par, 1:2, :]
                forward = jnp.where(where > b, moved, forward)
            for b in range(nsp - 1, 0, -1):
                off, par = place_of(jnp.int32(b))
                moved = ends[off, par, 2:3, :] * backward + ends[off, par, 3:4, :]
                backward = jnp.where(where < b, moved, backward)
            states[slot, 0:1, :] = forward
            states[slot, 1:2, :] = backward

    def leave(layer, slot, order, relays, waits):
        step = 32
        m = 3 * layer + 2

        def finish(i, _):
            at = pl.ds(pl.multiple_of(i * step, step), step)
            total = both[slot, at, :] + cums[0, slot, at, :] * states[slot, 0:1, :]
            total = total + cums[1, slot, at, :] * states[slot, 1:2, :]
            gate = gate_z[slot, at, :].astype(jnp.float32)
            mixed[at, :] = (total * gate * sigmoid(gate)).astype(jnp.bfloat16)
            return 0

        lax.fori_loop(0, rows // step, finish, 0)

        def use(_, kz, ky):
            term = lax.dot_general(
                mixed[...], weights[m, kz * ny + ky], (((1,), (1,)), ((), ())),
                preferred_element_type=jnp.float32,
            )
            owner = owner_of(kz, ky)
            t = div(owner, per)
            far = rem(div(t, 2) + nx - x, nx)
            other = rem(t + core, 2)
            at = pl.ds(pl.multiple_of(rem(owner, per) * depth, 128), depth)
            part[slot, other, far, :, at] = term.astype(jnp.bfloat16)

        if waits:
            own_weight(m).wait()
        walk(all_steps((m,), order), relays, waits, use)

    def s_to_core(slot, k, h):
        return remote(
            part.at[slot, 1, k, cut(h)], core_in.at[slot, k, cut(h)],
            sc_send.at[slot, k, h], sc_recv.at[slot, k, h], core_peer,
        )

    def s_to_x(slot, k, h):
        return remote(
            part.at[slot, 0, k, cut(h)], x_in.at[slot, k - 1, cut(h)],
            sx_send.at[slot, k - 1, h], sx_recv.at[slot, k - 1, h], x_peer(k),
        )

    def s_to_z(h, k=0):
        there = z_in.at[cut(h)] if k == 0 else x_in.at[1, k - 1, cut(h)]
        index = k * HALVES + h
        return remote(
            part.at[1, 0, k, cut(h)], there, sz_send.at[index], sz_recv.at[index], z_peer(1)
        )

    def give(slot):
        for h in range(HALVES):
            for k in list(range(1, nx)) + [0]:
                s_to_core(slot, k, h).start()

    def tiles(h, body):
        step = 32

        def run(i, _):
            body(pl.ds(pl.multiple_of(h * split + i * step, step), step))
            return 0

        lax.fori_loop(0, split // step, run, 0)

    def add_core(slot, k, h, more=None):
        def body(at):
            total = part[slot, 0, k, at, :].astype(jnp.float32)
            total = total + core_in[slot, k, at, :].astype(jnp.float32)
            if more is not None:
                total = total + more[at, :].astype(jnp.float32)
            part[slot, 0, k, at, :] = total.astype(jnp.bfloat16)

        tiles(h, body)

    def pass_on(slot, h):
        for k in range(1, nx):
            s_to_core(slot, k, h).wait_recv()
            add_core(slot, k, h)
            s_to_x(slot, k, h).start()
        s_to_core(slot, 0, h).wait_recv()

    def pass_over(h):
        for k in list(range(1, nx)) + [0]:
            s_to_core(1, k, h).wait_recv()
            add_core(1, k, h)
            s_to_z(h, k).start()

    def pass_joined(h):
        for k in range(1, nx):
            s_to_core(0, k, h).wait_recv()
            s_to_z(h, k).wait_recv()
            add_core(0, k, h, x_in.at[1, k - 1])
            s_to_x(0, k, h).start()
        s_to_core(0, 0, h).wait_recv()

    def summed(slot, at):
        total = part[slot, 0, 0, at, :].astype(jnp.float32)
        total = total + core_in[slot, 0, at, :].astype(jnp.float32)
        for k in range(1, nx):
            total = total + x_in[slot, k - 1, at, :].astype(jnp.float32)
        return total

    def land(slot, h):
        for k in range(1, nx):
            s_to_x(slot, k, h).wait_recv()

    def send_over(h):
        land(1, h)

        def body(at):
            part[1, 0, 0, at, :] = summed(1, at).astype(jnp.bfloat16)

        tiles(h, body)
        s_to_z(h).start()

    def renew(h, last):
        land(0, h)
        s_to_z(h).wait_recv()

        def body(at):
            total = summed(0, at) + z_in[at, :].astype(jnp.float32)
            fresh = (own[at, :].astype(jnp.float32) + total).astype(jnp.bfloat16)
            own[at, :] = fresh
            if not last:
                feats[0, column, at, :] = fresh

        tiles(h, body)

    def drain(crossed):
        for h in range(HALVES):
            for slot in range(2):
                for k in range(nx):
                    s_to_core(slot, k, h).wait_send()
                for k in range(1, nx):
                    if slot == 0 or h not in crossed:
                        s_to_x(slot, k, h).wait_send()
            s_to_z(h).wait_send()
            for k in range(1, nx):
                if h in crossed:
                    s_to_z(h, k).wait_send()

    first_own = pltpu.make_async_copy(stream_ref, own, start_sem.at[0])
    first_feat = pltpu.make_async_copy(stream_ref, feats.at[0, column], start_sem.at[1])
    channel = pl.multiple_of(column * 2 * width + role * width, 128)
    small = [
        pltpu.make_async_copy(taps_hbm.at[:, :, pl.ds(channel, width)], taps, start_sem.at[2]),
        pltpu.make_async_copy(rate_hbm.at[:, :, pl.ds(channel, width)], rate, start_sem.at[3]),
        pltpu.make_async_copy(
            gates_hbm.at[:, :, pl.ds(pl.multiple_of(role * width, 128), width), :],
            gates, start_sem.at[4],
        ),
    ]
    first_own.start()
    first_feat.start()
    pl.semaphore_wait(barrier, len(peers))
    order = [k for k in range(2, nz)] + [1]
    far = order[:-1]
    halves = range(HALVES)
    send_own_weights((0, 1))
    send_weights((0, far[0]))
    for h in halves:
        f_to_z(h, stream_ref).start()
        gather_start(h, stream_ref)
    send_weights(*[(0, k) for k in far[1:]], (0, 1), (1, far[0]), (1, 1))
    send_weights(*[(1, k) for k in far[1:]], (2, far[0]), (2, 1))
    for m in range(3 * layers):
        own_weight(m).start()
    for copy in small:
        copy.start()
    send_own_weights((2,))
    results = []

    for layer in range(layers):
        last = layer == layers - 1
        v, g, o = 3 * layer, 3 * layer + 1, 3 * layer + 2
        clear(layer)
        if layer == 0:
            gather_x(0, 0)
            relay(v, far[0])
            for h in range(1, HALVES):
                gather_x(0, h)
            for k in far[1:]:
                relay(v, k)
            for h in halves:
                gather_z(h)
            relay(v, 1)
            first_own.wait()
            first_feat.wait()
            for h in halves:
                gather_finish(0, h)
                normalize(layer, 0, h)
            relay(g, far[0])
            for h in halves:
                gather_x(1, h)
            relay(g, 1)
            for h in halves:
                gather_finish(1, h)
                normalize(layer, 1, h)
            inward = all_steps((v,), [0] + order)
            inward += all_steps((g,), [0, far[0], 1] + far[1:])
            enter(layer, (0, 1), inward, [(g, k) for k in far[1:]], True)
        else:
            relay(g, nth(0))
            for h in halves:
                gather_x(0, h)
                gather_z(h)

            @pl.when(role == 0)
            def _():
                for i in range(1, nz - 2):
                    relay(g, nth(i))

            @pl.when(role == 1)
            def _():
                send_weights((o, 1), *[(o, k) for k in reversed(far)])

            for h in halves:
                gather_finish(0, h)
                normalize(layer, 0, h)
            inward = all_steps((v,), [0] + order) + late_steps(g)
            middle = [(g, k) for k in range(2, nz - 1)]
            enter(layer, (0,), inward, [(g, nz - 1)], True, middle)
            relay(o, nth(0))
            for h in halves:
                gather_x(1, h)
            for h in halves:
                gather_finish(1, h)
                normalize(layer, 1, h)
            enter(layer, (1,), inward, [], False)
        edges_begin()
        if layer == 0:
            send_weights(*[(o, k) for k in far[1:]])
            relay(o, far[0])
            relay(o, 1)
        else:
            for i in range(1, nz - 2):
                relay(o, nth(i))
        edges_end()
        if layer == 0:
            for copy in small:
                copy.wait()
        if not last:
            send_weights((v + 3, 1))

            @pl.when(role == 1)
            def _():
                send_weights((v + 4, 1))

        scan(layer, [])
        ends_begin()
        if layer == 0:
            for k in far[1:]:
                relay(o, k)
        else:
            relay(o, nth(nz - 2))
        ends_end()
        if not last:
            send_weights(*[(v + 3, k) for k in far])

            @pl.when(role == 1)
            def _():
                send_weights(*[(v + 4, k) for k in reversed(far)])

            send_own_weights((v + 3, v + 4))
        leave(layer, 1, [0] + order, [], True)
        give(1)
        crossed = [h for h in halves if last and h >= (HALVES + 1) // 2]
        for h in halves:
            if h in crossed:
                pass_over(h)
            else:
                pass_on(1, h)
        leave(layer, 0, [0] + order, [], False)
        give(0)
        for h in halves:
            if h in crossed:
                pass_joined(h)
            else:
                pass_on(0, h)
        if not last:
            relay(v + 3, 1)
        for h in halves:
            if h not in crossed:
                send_over(h)
        if not last:

            @pl.when(role == 0)
            def _():
                send_weights((v + 4, far[0]))

            send_own_weights((v + 5,))
            relay(v + 3, far[0])
        for h in halves:
            renew(h, last)
            if not last:
                f_to_z(h, own).start()
                gather_start(h, own)
            else:
                result = pltpu.make_async_copy(
                    own.at[cut(h)], result_ref.at[cut(h)], out_sem.at[h]
                )
                result.start()
                results.append(result)
        if not last:
            for k in far[1:]:
                relay(v + 3, k)

            @pl.when(role == 0)
            def _():
                send_weights(*[(v + 4, k) for k in far[1:]], (v + 4, 1))
                send_weights(*[(v + 5, k) for k in far], (v + 5, 1))

        drain(crossed)
    for m in range(3 * layers):
        for k in range(1, nz):
            z_weight(m, k).wait_send()
        for kz in range(nz):
            for ky in range(1, ny):
                y_weight(m, kz, ky, kz == 0).wait_send()
    for result in results:
        result.wait()


def per_device(
    stream_in, norm_gain, value_proj, gate_proj, out_proj, conv_taps, block_gates, forget_rate
):
    nsp, ntp = lax.axis_size("sp"), lax.axis_size("tp")
    layers, depth, both_roles = value_proj.shape
    rows, size = stream_in.shape
    width = both_roles // 2
    block = block_gates.shape[-1]
    ny = 1 << ((nsp.bit_length() - 1) // 2)
    nz, nx, groups = nsp // ny, ntp // 2, nsp // 2
    maps = block_gates.reshape(layers, 4, both_roles, block)
    half, full = jnp.bfloat16, jnp.float32
    dma = pltpu.SemaphoreType.DMA
    slab = pltpu.VMEM((rows + 8 * CHUNKS, block), full)
    scratch = [
        pltpu.VMEM((2, ntp, rows, size), half),
        pltpu.VMEM((3 * layers, nsp, depth, width), half),
        pltpu.VMEM((rows, size), half),
        pltpu.VMEM((2, rows, width), half),
        pltpu.VMEM((2, rows, width), half),
        pltpu.VMEM((rows + 16, block), full),
        *[slab] * 8,
        pltpu.VMEM((2, rows, width), full),
        pltpu.VMEM((2, 2, rows, width), full),
        pltpu.VMEM((rows, width), half),
        pltpu.VMEM((2, 2, nx, rows, size), half),
        pltpu.VMEM((2, nx, rows, size), half),
        pltpu.VMEM((2, nx - 1, rows, size), half),
        pltpu.VMEM((rows, size), half),
        pltpu.VMEM((groups, 2, 16, width), full),
        pltpu.VMEM((groups, 2, 8, width), full),
        pltpu.VMEM((2, 8, width), full),
        pltpu.VMEM((layers, 4, width), full),
        pltpu.VMEM((layers, 4, width, block), half),
        pltpu.VMEM((layers, 2, width), full),
        dma((5,)),
        dma((3 * layers,)),
        dma((3 * layers, nz - 1)),
        dma((3 * layers, nz, ny - 1)),
        dma((3 * layers, nsp)),
        dma((HALVES,)), dma((HALVES,)),
        *[dma((2, nx - 1, HALVES))] * 2, *[dma((2, nx, HALVES))] * 2,
        dma((nx * HALVES,)), dma((nx * HALVES,)),
        *[dma((2, nx - 1, HALVES))] * 2, *[dma((2, nx, HALVES))] * 2,
        dma((groups - 1,)), dma((groups - 1,)), dma((groups - 1,)), dma((groups - 1,)),
        dma((HALVES,)),
    ]
    anywhere = pl.BlockSpec(memory_space=pl.ANY)
    inside = pl.BlockSpec(memory_space=pltpu.VMEM)
    return pl.pallas_call(
        functools.partial(kernel, nsp, ntp, layers),
        out_shape=jax.ShapeDtypeStruct((rows, size), half),
        in_specs=[anywhere] * 4 + [inside] + [anywhere] * 3,
        out_specs=anywhere,
        scratch_shapes=scratch,
        compiler_params=pltpu.CompilerParams(
            collective_id=0, has_side_effects=True, vmem_limit_bytes=VMEM_BYTES
        ),
        name="layers",
    )(stream_in, value_proj, gate_proj, out_proj, norm_gain, conv_taps, maps, forget_rate)


def solution(mesh):
    placed = (
        P("sp", "tp"),
        P(),
        P(None, "sp", "tp"),
        P(None, "sp", "tp"),
        P(None, "sp", "tp"),
        P(),
        P(None, None, None, "tp", None),
        P(),
    )
    return jax.shard_map(
        per_device, mesh=mesh, in_specs=placed, out_specs=P("sp", "tp"), check_vma=False
    )
```
